32 devices in a mesh: sp: 8 (over z, x), tp: 4 (over y, core).
Axes of the slice: x: 2, y: 2, z: 4, core: 2. Of those that a mesh axis runs over, the one named last changes fastest.
Arguments:
- cot_out: bfloat16 [2048, 2048], P('sp', 'tp'), may hold values from -6 to 6
- route_ids: int32 [2048, 2], P('sp'), may hold values from 0 to 7, all different within a row; in each aligned block of 256 rows (0 to 255, 256 to 511, ...) at most 96 rows name the same one
- route_weight: float32 [2048, 2], P('sp'), may hold values from 0.1 to 1
- expert_inputs: bfloat16 [8, 768, 2048], P('sp'), may hold values from -48 to 48
- w_gate: bfloat16 [8, 2048, 1024], P('sp', None, 'tp'), may hold values from -0.125 to 0.125
- w_up: bfloat16 [8, 2048, 1024], P('sp', None, 'tp'), may hold values from -0.125 to 0.125
- w_down: bfloat16 [8, 1024, 2048], P('sp', 'tp'), may hold values from -0.1875 to 0.1875
- w_proj: bfloat16 [2048, 2048], P('tp'), may hold values from -0.125 to 0.125
- conv_out: bfloat16 [2048, 2048], P('sp', 'tp'), may hold values from -6 to 6
- channel_norm_gain: float32 [2048], P('tp'), may hold values from 0.1 to 1.9
- taps: float32 [31, 2048], P(None, 'tp'), may hold values from -1 to 1
- value_pre: bfloat16 [2048, 2048], P('sp', 'tp'), may hold values from -6 to 6
- gate_pre: bfloat16 [2048, 2048], P('sp', 'tp'), may hold values from -6 to 6
Outputs:
- grad_gate_w: bfloat16 [8, 2048, 1024], P('sp', None, 'tp')
- grad_up_w: bfloat16 [8, 2048, 1024], P('sp', None, 'tp')
- grad_down_w: bfloat16 [8, 1024, 2048], P('sp', 'tp')
- grad_proj: float32 [2048, 2048], P(('tp', 'sp'))
- grad_value: bfloat16 [2048, 2048], P('sp', 'tp')
- grad_gate: bfloat16 [2048, 2048], P('sp', 'tp')
The draws below stay inside these ranges and needn't reach their ends.
Inputs may be any that keep to these rules, and one draw needn't show every extreme that they name: `route_ids`: among the tokens of one index of sp no expert is chosen more than 96 times, a bound that some block reaches; a token's experts differ.
All inputs are finite; a program needn't handle non-finite values.
Results may differ from the reference program's by a relative error of at most 0.012.
Values may be sent and summed in bfloat16 or wider, within the bound.
A program may use at most 128 MiB of HBM per device.

```python
import math
import jax
import jax.numpy as jnp
import numpy as np
from jax import lax

D = 2048
F = 1024
WIDTH = 31
TOP = 2
TOK_DEV = 256
EXPERTS = 8
CAP = 96
SLOTS = 768
TOKENS = 2048
N_SP = 8
N_TP = 4


def draw_expert_inputs(key, part):
    keys = jax.random.split(jax.random.fold_in(key, 11), 2)
    shape = (EXPERTS, SLOTS, D)
    base = jax.random.truncated_normal(keys[0], -6.0, 6.0, shape, jnp.float32)
    scales = jnp.exp(jax.random.uniform(keys[1], (EXPERTS, SLOTS, 1), jnp.float32, jnp.log(0.5), jnp.log(6.0)))
    values = scales * base
    return jnp.clip(values, -48.0, 48.0).astype(jnp.bfloat16)


def spiked(values, own_key, source, target, parts, factor):
    def block_of(position):
        return (jnp.arange(values.shape[position]) // (values.shape[position] // parts)).reshape((-1,) + (1,) * (values.ndim - 1 - position))

    near = jax.random.permutation(own_key, parts)[block_of(target)]
    second = (block_of(target) + parts // 2) % parts
    return jnp.where((block_of(source) == near) | (block_of(source) == second), factor * values, values)


def level_of(own_key, dims, pieces, least, top_value):
    def one(axis_at, blocks):
        draws = jax.random.uniform(jax.random.fold_in(jax.random.fold_in(own_key, 6), axis_at), (blocks,), jnp.float32, least / len(pieces), top_value / len(pieces))
        return jnp.repeat(jnp.exp(draws), dims[axis_at] // blocks).reshape((-1,) + (1,) * (len(dims) - axis_at - 1))

    gain = one(*pieces[0])
    for cut in pieces[1:]:
        gain = gain * one(*cut)
    return gain


def shared_out(stream_key, own, number, rows, count, top, reach, lean):
    ranking = jax.random.permutation(stream_key, count)
    heavy_load, usual = shares(count, rows * top, reach, lean, True), shares(count, rows * top, reach, lean, False)
    places = jnp.arange(count)

    def named(tallies, offset_by):
        used = int((tallies > 0).sum())
        fixed = max(1, used // 4)
        passed = fixed + (places - fixed + offset_by * (used - fixed)) % max(1, count - fixed)
        return jnp.zeros((count,), jnp.int32).at[ranking[jnp.where(places < fixed, places, passed)]].set(jnp.asarray(tallies, jnp.int32))

    tallies = jnp.where(number % 4 == 0, named(heavy_load, number // 4), named(usual, number - number // 4 - 1))
    mixed = jax.random.permutation(jax.random.fold_in(own, 3), count)
    source_of, sink = mixed[0:count // 2 * 2:2], mixed[1:count // 2 * 2:2]
    room = jnp.minimum(tallies[source_of] - 1, reach - tallies[sink]) // 2
    room = jnp.where((source_of == ranking[0]) | (sink == ranking[0]) | (tallies[sink] == 0), 0, jnp.maximum(room, 0))
    passed = jax.random.randint(jax.random.fold_in(own, 4), (count // 2,), 0, 1 << 20) % (room + 1)
    tallies = tallies.at[source_of].add(-passed).at[sink].add(passed)
    members = jnp.searchsorted(jnp.cumsum(tallies), jnp.arange(rows * top), side="right").astype(jnp.int32)
    table = members.reshape(top, rows).T
    table = table[jax.random.permutation(jax.random.fold_in(own, 1), rows)]
    offset_by = jax.random.randint(jax.random.fold_in(own, 2), (rows, 1), 0, top)
    return jnp.take_along_axis(table, (jnp.arange(top)[None, :] + offset_by) % top, axis=1)


def shares(amount, total, limit, lean, full):
    portions = [(1 << 20) // math.isqrt(grade ** lean) + 1 for grade in range(1, amount + 1)]
    largest = limit if full else min(limit, max(-(-total // amount), total * portions[0] // sum(portions)))
    least = 1 if total - largest >= amount - 1 else 0
    given, rest = [largest] + [least] * (amount - 1), total - largest - least * (amount - 1)
    while rest > 0:
        free = [i for i in range(1, amount) if given[i] < largest] or [i for i in range(1, amount) if given[i] < limit]
        whole, budget = sum([portions[i] for i in free]), rest
        for i in free:
            extra = min(limit - given[i], max(1, budget * portions[i] // whole), rest)
            given[i] = given[i] + extra
            rest = rest - extra
    return np.array(given)


def centred(key, dims, width, most, cuts=(), held_as=jnp.bfloat16):
    drawn = jax.random.normal(key, dims, jnp.float32) * width
    if len(cuts) > 0:
        drawn = level_of(key, dims, cuts, -0.22, 0.18) * drawn
    return jnp.clip(drawn, min=-most, max=most).astype(held_as)


def gaussian_with(key, shape, spread, reach, shards, heavy, held_as=jnp.bfloat16):
    drawn = spread * jax.random.normal(key, shape, jnp.float32)
    if shards:
        drawn = drawn * level_of(key, shape, shards, -0.22, 0.18)
    return jnp.clip(spiked(drawn, jax.random.fold_in(key, 3), *heavy), -reach, reach).astype(held_as)


def setup_inputs(seed: int = 0) -> dict:
    seeds = jax.random.split(jax.random.key(seed), 14)
    cot_out = gaussian_with(seeds[0], (TOKENS, D), 1.0, 6.0, ((0, 8), (1, 4)), (0, 1, 8, 2.0))
    route_ids_keys = jax.random.split(jax.random.fold_in(seeds[1], 1), TOKENS // TOK_DEV)
    route_ids_turns = jax.random.permutation(jax.random.fold_in(seeds[1], 3), TOKENS // TOK_DEV)
    route_ids = jax.vmap(lambda own, number: shared_out(jax.random.fold_in(seeds[1], 2), own, number, TOK_DEV, EXPERTS, TOP, CAP, 2))(route_ids_keys, route_ids_turns).reshape((TOKENS, TOP))
    route_weight = jnp.clip(jnp.exp(math.log(1.0) - 2.3025851 * jax.random.uniform(seeds[2], (TOKENS, TOP), jnp.float32) ** level_of(seeds[2], (TOKENS, TOP), ((0, 8),), -0.2, 0.2)), 0.1, 1.0)
    expert_inputs = draw_expert_inputs(jax.random.fold_in(seeds[13], 71), 0)
    w_gate = centred(seeds[4], (EXPERTS, D, F), D ** -0.5, 0.125, ((0, 8), (2, 4)))
    w_up = centred(seeds[5], (EXPERTS, D, F), D ** -0.5, 0.125, ((0, 8), (2, 4)))
    w_down = centred(seeds[6], (EXPERTS, F, D), F ** -0.5, 0.1875, ((0, 8), (1, 4)))
    w_proj = centred(seeds[7], (D, D), D ** -0.5, 0.125, ((0, 4),))
    conv_out = centred(seeds[8], (TOKENS, D), 1.0, 6.0, ((0, 8), (1, 4)))
    channel_norm_gain = jnp.clip(1.0 + 0.18 * jax.random.normal(seeds[9], (D,), jnp.float32), 0.1, 1.9)
    taps = centred(seeds[10], (WIDTH, D), WIDTH ** -0.5, 1.0, ((1, 4),), jnp.float32)
    value_pre = centred(seeds[11], (TOKENS, D), 1.0, 6.0, ((0, 8), (1, 4)))
    gate_pre = centred(seeds[12], (TOKENS, D), 1.5, 6.0, ((0, 8), (1, 4)))
    return dict(cot_out=cot_out, route_ids=route_ids, route_weight=route_weight, expert_inputs=expert_inputs, w_gate=w_gate, w_up=w_up, w_down=w_down, w_proj=w_proj, conv_out=conv_out, channel_norm_gain=channel_norm_gain, taps=taps, value_pre=value_pre, gate_pre=gate_pre)


clamp_limit = 7.0
swish_alpha = 1.702
norm_epsilon = 1e-05

def one_expert(operands):
    rows_in, rows_cot, gate_weight, up_weight, down_weight = operands
    gate_lin = jnp.dot(rows_in, gate_weight, preferred_element_type=jnp.float32)
    up_lin = jnp.dot(rows_in, up_weight, preferred_element_type=jnp.float32)
    gate_c = jnp.minimum(gate_lin, clamp_limit)
    up_c = jnp.clip(up_lin, -clamp_limit, clamp_limit)
    sig = jax.nn.sigmoid(swish_alpha * gate_c)
    act = ((up_c + 1.0) * gate_c * sig).astype(jnp.bfloat16)
    grad_down = jnp.dot(act.T, rows_cot, preferred_element_type=jnp.float32).astype(jnp.bfloat16)
    d_act = jnp.dot(rows_cot, down_weight.T, preferred_element_type=jnp.float32)
    up_open = ((up_lin > -clamp_limit) & (up_lin < clamp_limit)).astype(jnp.float32)
    gate_open = (gate_lin < clamp_limit).astype(jnp.float32)
    d_up = (d_act * gate_c * sig * up_open).astype(jnp.bfloat16)
    d_gate = (d_act * (up_c + 1.0) * (sig + swish_alpha * gate_c * sig * (1.0 - sig)) * gate_open).astype(jnp.bfloat16)
    grad_gate = jnp.dot(rows_in.T, d_gate, preferred_element_type=jnp.float32).astype(jnp.bfloat16)
    grad_up = jnp.dot(rows_in.T, d_up, preferred_element_type=jnp.float32).astype(jnp.bfloat16)
    blocks = F // N_TP
    gate_parts = jnp.einsum('snf,dnf->nsd', d_gate.reshape(SLOTS, N_TP, blocks).astype(jnp.float32), gate_weight.reshape(D, N_TP, blocks).astype(jnp.float32))
    up_parts = jnp.einsum('snf,dnf->nsd', d_up.reshape(SLOTS, N_TP, blocks).astype(jnp.float32), up_weight.reshape(D, N_TP, blocks).astype(jnp.float32))
    rounded = (gate_parts + up_parts).astype(jnp.bfloat16)
    rounded = lax.optimization_barrier(rounded)
    input_grad = lax.optimization_barrier(jnp.sum(rounded.astype(jnp.float32), axis=0)).astype(jnp.bfloat16)
    return (grad_gate, grad_up, grad_down, input_grad)

def reference(cot_out, route_ids, route_weight, expert_inputs, w_gate, w_up, w_down, w_proj, conv_out, channel_norm_gain, taps, value_pre, gate_pre):
    block_ids = route_ids.reshape(N_SP, TOK_DEV * TOP)
    expert_hot = (block_ids[:, :, None] == jnp.arange(EXPERTS, dtype=jnp.int32)[None, None, :]).astype(jnp.int32)
    earlier = lax.optimization_barrier(jnp.sum((jnp.cumsum(expert_hot, axis=1) - expert_hot) * expert_hot, axis=2))
    dest_slot = (jnp.arange(N_SP, dtype=jnp.int32)[:, None] * CAP + earlier).reshape(-1).astype(jnp.int32)
    expert_of = block_ids.reshape(-1).astype(jnp.int32)
    repeated = jnp.repeat(cot_out, TOP, axis=0).astype(jnp.float32)
    scaled = (route_weight.reshape(-1)[:, None] * repeated).astype(jnp.bfloat16)
    expert_cot = jnp.zeros((EXPERTS, SLOTS, D), jnp.bfloat16).at[expert_of, dest_slot].set(scaled)
    grad_gate_w, grad_up_w, grad_down_w, expert_grad = lax.map(one_expert, (expert_inputs, expert_cot, w_gate, w_up, w_down))
    picked = expert_grad[expert_of, dest_slot].astype(jnp.float32).reshape(TOKENS, TOP, D)
    mix_grad = (cot_out.astype(jnp.float32) + lax.optimization_barrier(jnp.sum(picked, axis=1))).astype(jnp.bfloat16)
    convolution_filter = conv_out.astype(jnp.float32)
    channel_mean = lax.optimization_barrier(jnp.mean(convolution_filter, axis=1, keepdims=True))
    var = lax.optimization_barrier(jnp.mean(convolution_filter * convolution_filter, axis=1, keepdims=True)) - channel_mean * channel_mean
    inverse_deviation = lax.rsqrt(var + norm_epsilon)
    normalized_input = (convolution_filter - channel_mean) * inverse_deviation
    normalized_output = normalized_input * channel_norm_gain[None, :]
    sig = jax.nn.sigmoid(normalized_output)
    act_conv = (normalized_output * sig).astype(jnp.bfloat16)
    grad_proj = jnp.dot(act_conv.T, mix_grad, preferred_element_type=jnp.float32)
    d_act_conv = jnp.dot(mix_grad, w_proj.T, preferred_element_type=jnp.float32)
    normalized_gradient = d_act_conv * sig * (1.0 + normalized_output * (1.0 - sig)) * channel_norm_gain[None, :]
    first_moment_mean = lax.optimization_barrier(jnp.mean(normalized_gradient, axis=1, keepdims=True))
    second_moment_mean = lax.optimization_barrier(jnp.mean(normalized_gradient * normalized_input, axis=1, keepdims=True))
    convolution_gradient = inverse_deviation * (normalized_gradient - first_moment_mean - normalized_input * second_moment_mean)
    extended = jnp.concatenate([convolution_gradient, jnp.zeros((WIDTH - 1, D), jnp.float32)], axis=0)
    d_glu = jnp.zeros((TOKENS, D), jnp.float32)
    for offset in range(WIDTH):
        begin = WIDTH - 1 - offset
        d_glu = d_glu + taps[offset][None, :] * extended[begin:begin + TOKENS]
    gate_sig = jax.nn.sigmoid(gate_pre.astype(jnp.float32))
    grad_value = (d_glu * gate_sig).astype(jnp.bfloat16)
    grad_gate = (d_glu * value_pre.astype(jnp.float32) * gate_sig * (1.0 - gate_sig)).astype(jnp.bfloat16)
    return (grad_gate_w, grad_up_w, grad_down_w, grad_proj, grad_value, grad_gate)
```

```python
import functools

import jax
import jax.numpy as jnp
from jax import lax
from jax.experimental import pallas as pl
from jax.experimental.pallas import tpu as pltpu
from jax.sharding import PartitionSpec as P

clamp_limit = 7.0
swish_alpha = 1.702
norm_epsilon = 1e-05
MESH = pl.DeviceIdType.MESH
VMEM = pltpu.VMEM


def passed_along(value, axis, steps):
    count = lax.axis_size(axis)
    leading, last = (max(0, -steps), min(count, count - steps))
    return lax.ppermute(value, axis, [(source, source + steps) for source in range(leading, last)])


def lanes(index, width):
    return pl.ds(pl.multiple_of(index * width, width), width)


def places(group, narrow):
    me, t = lax.axis_index("sp"), lax.axis_index("tp")
    near = t + 1 - 2 * lax.rem(t, 2)
    far = lax.rem(t + narrow // 2, narrow)
    return me, t, near, far, lax.rem(near + narrow // 2, narrow)


def remote(src, dst, send, recv, sp, tp):
    return pltpu.make_async_remote_copy(
        src_ref=src, dst_ref=dst, send_sem=send, recv_sem=recv, device_id=(sp, tp), device_id_type=MESH
    )


def meet(peers):
    barrier = pltpu.get_barrier_semaphore()
    for sp, tp in peers:
        pl.semaphore_signal(barrier, inc=1, device_id=(sp, tp), device_id_type=MESH)
    pl.semaphore_wait(barrier, len(peers))


def dispatch_kernel(group, narrow, width, out_ref, stat_ref, rows_ref, stats_ref, *sems):
    a_s, a_r, n_s, n_r, f_s, f_r, m_s, m_r, t_s, t_r, l_s = sems
    me, t, near, far, cross = places(group, narrow)
    sp_peers = [lax.rem(me + o, group) for o in range(1, group)]
    meet([(p, t) for p in sp_peers] + [(me, near), (me, far), (me, cross)])

    def spot(s, column):
        return rows_ref.at[s, :, lanes(column, width)]

    def swap(s):
        return remote(out_ref.at[s], spot(me, t), a_s.at[s], a_r.at[me], s, t)

    for p in sp_peers:
        swap(p).start()
    stat_own = pltpu.make_async_copy(stat_ref, stats_ref.at[t], l_s.at[0])
    stat_own.start()
    small = []
    for k, p in enumerate((near, far, cross)):
        c = remote(stat_ref, stats_ref.at[t], t_s.at[k], t_r.at[k], me, p)
        c.start()
        small.append(c)
    own = pltpu.make_async_copy(out_ref.at[me], spot(me, t), l_s.at[1])
    own.start()
    own.wait()
    order = [me] + [lax.rem(me + group - o, group) for o in range(1, group)]

    def to_far(s):
        return remote(spot(s, t), spot(s, t), f_s.at[s], f_r.at[s], me, far)

    def to_near(s):
        return remote(spot(s, t), spot(s, t), n_s.at[s], n_r.at[s], me, near)

    def onward(s):
        return remote(spot(s, far), spot(s, far), m_s.at[s], m_r.at[s], me, near)

    for i, s in enumerate(order):
        if i > 0:
            remote(out_ref.at[s], spot(s, t), a_s.at[s], a_r.at[s], s, t).wait_recv()
        to_far(s).start()
        to_near(s).start()
        if i > 0:
            prev = order[i - 1]
            remote(spot(prev, far), spot(prev, far), f_s.at[prev], f_r.at[prev], me, far).wait_recv()
            onward(prev).start()
    last = order[-1]
    remote(spot(last, far), spot(last, far), f_s.at[last], f_r.at[last], me, far).wait_recv()
    onward(last).start()
    for s in order:
        to_far(s).wait_send()
        to_near(s).wait_send()
        onward(s).wait_send()
        remote(spot(s, near), spot(s, near), n_s.at[s], n_r.at[s], me, near).wait_recv()
        remote(spot(s, cross), spot(s, cross), m_s.at[s], m_r.at[s], me, near).wait_recv()
    for p in sp_peers:
        swap(p).wait_send()
    stat_own.wait()
    for c in small:
        c.wait_send()
        c.wait_recv()


def dispatch(outgoing, stat):
    group, capacity, width = outgoing.shape
    narrow = lax.axis_size("tp")
    dma = pltpu.SemaphoreType.DMA
    return pl.pallas_call(
        functools.partial(dispatch_kernel, group, narrow, width),
        out_shape=(
            jax.ShapeDtypeStruct((group, capacity, narrow * width), outgoing.dtype),
            jax.ShapeDtypeStruct((narrow,) + stat.shape, stat.dtype),
        ),
        in_specs=[pl.BlockSpec(memory_space=VMEM)] * 2,
        out_specs=[pl.BlockSpec(memory_space=VMEM)] * 2,
        scratch_shapes=[dma((group,))] * 8 + [dma((3,))] * 2 + [dma((2,))],
        compiler_params=pltpu.CompilerParams(collective_id=0, has_side_effects=True),
    )(outgoing, stat)


def return_kernel(group, narrow, width, part_ref, home_ref, pair_buf, far_out, far_in, done, *sems):
    n_s, n_r, f_s, f_r, a_s, a_r, l_s = sems
    me, t, near, far, cross = places(group, narrow)
    sp_peers = [lax.rem(me + o, group) for o in range(1, group)]
    meet([(p, t) for p in sp_peers] + [(me, near), (me, far)])
    order = sp_peers + [me]

    def part(s, column):
        return part_ref.at[s, :, lanes(column, width)]

    def to_near(s, k):
        return remote(
            part(s, near if k == 0 else cross), pair_buf.at[s, k], n_s.at[s, k], n_r.at[s, k], me, near
        )

    def to_far(s):
        return remote(far_out.at[s], far_in.at[s], f_s.at[s], f_r.at[s], me, far)

    def to_home(s):
        return remote(done.at[s], home_ref.at[me], a_s.at[s], a_r.at[me], s, t)

    for s in order:
        to_near(s, 1).start()
        to_near(s, 0).start()
    own = pltpu.make_async_copy(done.at[me], home_ref.at[me], l_s.at[0])

    def finish(s, i):
        to_near(s, 0).wait_recv()
        to_far(s).wait_recv()
        total = part_ref[s, :, lanes(t, width)].astype(jnp.float32)
        total = total + pair_buf[s, 0].astype(jnp.float32) + far_in[s].astype(jnp.float32)
        done[s] = total.astype(done.dtype)
        if i < group - 1:
            to_home(s).start()
        else:
            own.start()

    lag = min(2, group - 1)
    for i, s in enumerate(order):
        to_near(s, 1).wait_recv()
        pair = part_ref[s, :, lanes(far, width)].astype(jnp.float32) + pair_buf[s, 1].astype(jnp.float32)
        far_out[s] = pair.astype(far_out.dtype)
        to_far(s).start()
        if i >= lag:
            finish(order[i - lag], i - lag)
    for i in range(group - lag, group):
        finish(order[i], i)
    own.wait()
    for s in order:
        to_near(s, 0).wait_send()
        to_near(s, 1).wait_send()
        to_far(s).wait_send()
    for s in sp_peers:
        to_home(s).wait_send()
        remote(done.at[s], home_ref.at[s], a_s.at[s], a_r.at[s], s, t).wait_recv()


def return_home(partial):
    group, capacity, whole = partial.shape
    narrow = lax.axis_size("tp")
    width = whole // narrow
    dma = pltpu.SemaphoreType.DMA
    block = (group, capacity, width)
    return pl.pallas_call(
        functools.partial(return_kernel, group, narrow, width),
        out_shape=jax.ShapeDtypeStruct(block, partial.dtype),
        in_specs=[pl.BlockSpec(memory_space=VMEM)],
        out_specs=pl.BlockSpec(memory_space=VMEM),
        scratch_shapes=[
            VMEM((group, 2, capacity, width), partial.dtype),
            VMEM(block, partial.dtype),
            VMEM(block, partial.dtype),
            VMEM(block, partial.dtype),
        ]
        + [dma((group, 2))] * 2
        + [dma((group,))] * 4
        + [dma((1,))],
        compiler_params=pltpu.CompilerParams(collective_id=1, has_side_effects=True),
    )(partial)


def widen_kernel(narrow, width, pieces, mix_ref, full_ref, *sems):
    n_s, n_r, f_s, f_r, m_s, m_r, l_s = sems
    me, t, near, far, cross = places(1, narrow)
    meet([(me, near), (me, far)])
    rows = mix_ref.shape[0] // pieces

    def src(k):
        return mix_ref.at[pl.ds(k * rows, rows)]

    def spot(k, column):
        return full_ref.at[pl.ds(k * rows, rows), lanes(column, width)]

    def to_far(k):
        return remote(src(k), spot(k, t), f_s.at[k], f_r.at[k], me, far)

    def to_near(k):
        return remote(src(k), spot(k, t), n_s.at[k], n_r.at[k], me, near)

    def onward(k):
        return remote(spot(k, far), spot(k, far), m_s.at[k], m_r.at[k], me, near)

    own = pltpu.make_async_copy(mix_ref, full_ref.at[:, lanes(t, width)], l_s.at[0])
    for k in range(pieces):
        to_far(k).start()
    for k in range(pieces):
        to_near(k).start()
    own.start()
    for k in range(pieces):
        to_far(k).wait_recv()
        onward(k).start()
    own.wait()
    for k in range(pieces):
        to_far(k).wait_send()
        to_near(k).wait()
        onward(k).wait()


def widen(mix):
    rows, width = mix.shape
    narrow = lax.axis_size("tp")
    pieces = 4
    dma = pltpu.SemaphoreType.DMA
    return pl.pallas_call(
        functools.partial(widen_kernel, narrow, width, pieces),
        out_shape=jax.ShapeDtypeStruct((rows, narrow * width), mix.dtype),
        in_specs=[pl.BlockSpec(memory_space=VMEM)],
        out_specs=pl.BlockSpec(memory_space=VMEM),
        scratch_shapes=[dma((pieces,))] * 6 + [dma((1,))],
        compiler_params=pltpu.CompilerParams(collective_id=2, has_side_effects=True),
    )(mix)


def per_device(
    cot_out,
    route_ids,
    route_weight,
    expert_inputs,
    w_gate,
    w_up,
    w_down,
    w_proj,
    conv_out,
    channel_norm_gain,
    taps,
    value_pre,
    gate_pre,
):
    group_size = lax.axis_size("sp")
    narrow_size = lax.axis_size("tp")
    tok_rows, local_cols = cot_out.shape
    chosen = route_ids.shape[1]
    slot_rows = expert_inputs.shape[1]
    capacity = slot_rows // group_size
    model_width = expert_inputs.shape[2]
    f32, bf16 = jnp.float32, jnp.bfloat16
    experts = jnp.arange(group_size, dtype=jnp.int32)[None, :]
    hots = [(route_ids[:, k : k + 1] == experts) for k in range(chosen)]
    hot = functools.reduce(jnp.logical_or, hots)
    token = jnp.arange(tok_rows, dtype=jnp.int32)
    before = (token[:, None] > token[None, :]).astype(bf16)
    earlier = jnp.dot(before, hot.astype(bf16), preferred_element_type=f32)
    slots = jnp.arange(slot_rows, dtype=jnp.int32)[None, :]
    picks, scaled = [], []
    for k in range(chosen):
        slot = jnp.sum(jnp.where(hots[k], earlier, 0.0), axis=1).astype(jnp.int32)
        dest = route_ids[:, k] * capacity + slot
        picks.append((dest[:, None] == slots).astype(bf16))
        scaled.append((route_weight[:, k : k + 1] * cot_out.astype(f32)).astype(bf16))
    outgoing = lax.dot_general(
        jnp.concatenate(picks, axis=0),
        jnp.concatenate(scaled, axis=0),
        (((0,), (0,)), ((), ())),
        preferred_element_type=f32,
    ).astype(bf16)
    convolution_filter = conv_out.astype(f32)
    stat = jnp.stack(
        [jnp.sum(convolution_filter, axis=1), jnp.sum(convolution_filter * convolution_filter, axis=1)]
    )
    arrived, stats = dispatch(outgoing.reshape(group_size, capacity, local_cols), stat)
    rows_cot = arrived.reshape(slot_rows, model_width)
    rows_in = expert_inputs[0]
    gate_weight = w_gate[0]
    up_weight = w_up[0]
    down_weight = w_down[0]
    gate_lin = jnp.dot(rows_in, gate_weight, preferred_element_type=f32)
    up_lin = jnp.dot(rows_in, up_weight, preferred_element_type=f32)
    gate_c = jnp.minimum(gate_lin, clamp_limit)
    up_c = jnp.clip(up_lin, -clamp_limit, clamp_limit)
    sigma = jax.nn.sigmoid(swish_alpha * gate_c)
    act = ((up_c + 1.0) * gate_c * sigma).astype(bf16)
    grad_down = jnp.dot(act.T, rows_cot, preferred_element_type=f32).astype(bf16)
    d_act = jnp.dot(rows_cot, down_weight.T, preferred_element_type=f32)
    up_open = ((up_lin > -clamp_limit) & (up_lin < clamp_limit)).astype(f32)
    gate_open = (gate_lin < clamp_limit).astype(f32)
    d_up = (d_act * gate_c * sigma * up_open).astype(bf16)
    d_gate = (
        d_act * (up_c + 1.0) * (sigma + swish_alpha * gate_c * sigma * (1.0 - sigma)) * gate_open
    ).astype(bf16)
    grad_gate_part = jnp.dot(rows_in.T, d_gate, preferred_element_type=f32).astype(bf16)
    grad_up_part = jnp.dot(rows_in.T, d_up, preferred_element_type=f32).astype(bf16)
    partial_value = jnp.dot(d_gate, gate_weight.T, preferred_element_type=f32)
    partial_value = partial_value + jnp.dot(d_up, up_weight.T, preferred_element_type=f32)
    coming = return_home(partial_value.astype(bf16).reshape(group_size, capacity, model_width))
    pick_any = functools.reduce(jnp.add, picks)
    summed = jnp.dot(pick_any, coming.reshape(slot_rows, local_cols), preferred_element_type=f32)
    mix_grad = (cot_out.astype(f32) + summed).astype(bf16)
    mix_full = widen(mix_grad)
    channel_total = local_cols * narrow_size
    first_sum, square_sum = jnp.sum(stats, axis=0)
    channel_mean = (first_sum / channel_total)[:, None]
    var = (square_sum / channel_total)[:, None] - channel_mean * channel_mean
    inverse_deviation = lax.rsqrt(var + norm_epsilon)
    normalized_input = (convolution_filter - channel_mean) * inverse_deviation
    normalized_output = normalized_input * channel_norm_gain[None, :]
    sigma_conv = jax.nn.sigmoid(normalized_output)
    act_conv = (normalized_output * sigma_conv).astype(bf16)
    grad_proj = lax.psum_scatter(
        lax.dot_general(act_conv, mix_full, (((0,), (0,)), ((), ())), preferred_element_type=f32).astype(
            bf16
        ),
        "sp",
        scatter_dimension=0,
        tiled=True,
    ).astype(f32)
    d_act_conv = jnp.dot(mix_full, w_proj.T, preferred_element_type=f32)
    normalized_gradient = (
        d_act_conv
        * sigma_conv
        * (1.0 + normalized_output * (1.0 - sigma_conv))
        * channel_norm_gain[None, :]
    )
    first_term_gradient, second_term_gradient = lax.psum(
        (
            jnp.sum(normalized_gradient, axis=1),
            jnp.sum(normalized_gradient * normalized_input, axis=1),
        ),
        "tp",
    )
    convolution_gradient = inverse_deviation * (
        normalized_gradient
        - (first_term_gradient / channel_total)[:, None]
        - normalized_input * (second_term_gradient / channel_total)[:, None]
    )
    reach = taps.shape[0]
    following = passed_along(convolution_gradient[: reach - 1], "sp", -1)
    extended = jnp.concatenate([convolution_gradient, following], axis=0)
    d_glu = jnp.zeros_like(convolution_gradient)
    for offset in range(reach):
        begin = reach - 1 - offset
        d_glu = d_glu + taps[offset][None, :] * extended[begin : begin + tok_rows]
    gate_sig = jax.nn.sigmoid(gate_pre.astype(f32))
    grad_value = (d_glu * gate_sig).astype(bf16)
    grad_gate = (d_glu * value_pre.astype(f32) * gate_sig * (1.0 - gate_sig)).astype(bf16)
    return (
        grad_gate_part[None],
        grad_up_part[None],
        grad_down[None],
        grad_proj,
        grad_value,
        grad_gate,
    )


def solution(mesh):
    return jax.shard_map(
        per_device,
        mesh=mesh,
        in_specs=(
            P("sp", "tp"),
            P("sp", None),
            P("sp", None),
            P("sp", None, None),
            P("sp", None, "tp"),
            P("sp", None, "tp"),
            P("sp", "tp", None),
            P("tp", None),
            P("sp", "tp"),
            P("tp"),
            P(None, "tp"),
            P("sp", "tp"),
            P("sp", "tp"),
        ),
        out_specs=(
            P("sp", None, "tp"),
            P("sp", None, "tp"),
            P("sp", "tp", None),
            P(("tp", "sp"), None),
            P("sp", "tp"),
            P("sp", "tp"),
        ),
        check_vma=False,
    )
```

```python
import functools

import jax
import jax.numpy as jnp
from jax import lax
from jax.experimental import pallas as pl
from jax.experimental.pallas import tpu as pltpu
from jax.sharding import PartitionSpec as P

clamp_limit = 7.0
swish_alpha = 1.702
norm_epsilon = 1e-05
MESH = pl.DeviceIdType.MESH
VMEM = pltpu.VMEM


def lanes(index, width):
    return pl.ds(pl.multiple_of(index * width, width), width)


def places(group, narrow):
    me, t = lax.axis_index("sp"), lax.axis_index("tp")
    near = t + 1 - 2 * lax.rem(t, 2)
    far = lax.rem(t + narrow // 2, narrow)
    return me, t, near, far, lax.rem(near + narrow // 2, narrow)


def remote(src, dst, send, recv, sp, tp):
    return pltpu.make_async_remote_copy(
        src_ref=src, dst_ref=dst, send_sem=send, recv_sem=recv, device_id=(sp, tp), device_id_type=MESH
    )


def meet(peers):
    barrier = pltpu.get_barrier_semaphore()
    for sp, tp in peers:
        pl.semaphore_signal(barrier, inc=1, device_id=(sp, tp), device_id_type=MESH)
    pl.semaphore_wait(barrier, len(peers))


def dispatch_kernel(group, narrow, width, out_ref, stat_ref, rows_ref, stats_ref, *sems):
    a_s, a_r, n_s, n_r, f_s, f_r, m_s, m_r, t_s, t_r, l_s = sems
    me, t, near, far, cross = places(group, narrow)
    sp_peers = [lax.rem(me + o, group) for o in range(1, group)]
    meet([(p, t) for p in sp_peers] + [(me, near), (me, far), (me, cross)])

    def spot(s, column):
        return rows_ref.at[s, :, lanes(column, width)]

    def swap(s):
        return remote(out_ref.at[s], spot(me, t), a_s.at[s], a_r.at[me], s, t)

    for p in sp_peers:
        swap(p).start()
    stat_own = pltpu.make_async_copy(stat_ref, stats_ref.at[t], l_s.at[0])
    stat_own.start()
    small = []
    for k, p in enumerate((near, far, cross)):
        c = remote(stat_ref, stats_ref.at[t], t_s.at[k], t_r.at[k], me, p)
        c.start()
        small.append(c)
    own = pltpu.make_async_copy(out_ref.at[me], spot(me, t), l_s.at[1])
    own.start()
    own.wait()
    order = [me] + [lax.rem(me + group - o, group) for o in range(1, group)]

    def to_far(s):
        return remote(spot(s, t), spot(s, t), f_s.at[s], f_r.at[s], me, far)

    def to_near(s):
        return remote(spot(s, t), spot(s, t), n_s.at[s], n_r.at[s], me, near)

    def onward(s):
        return remote(spot(s, far), spot(s, far), m_s.at[s], m_r.at[s], me, near)

    for i, s in enumerate(order):
        if i > 0:
            remote(out_ref.at[s], spot(s, t), a_s.at[s], a_r.at[s], s, t).wait_recv()
        to_far(s).start()
        to_near(s).start()
        if i > 0:
            prev = order[i - 1]
            remote(spot(prev, far), spot(prev, far), f_s.at[prev], f_r.at[prev], me, far).wait_recv()
            onward(prev).start()
    last = order[-1]
    remote(spot(last, far), spot(last, far), f_s.at[last], f_r.at[last], me, far).wait_recv()
    onward(last).start()
    for s in order:
        to_far(s).wait_send()
        to_near(s).wait_send()
        onward(s).wait_send()
        remote(spot(s, near), spot(s, near), n_s.at[s], n_r.at[s], me, near).wait_recv()
        remote(spot(s, cross), spot(s, cross), m_s.at[s], m_r.at[s], me, near).wait_recv()
    for p in sp_peers:
        swap(p).wait_send()
    stat_own.wait()
    for c in small:
        c.wait_send()
        c.wait_recv()


def dispatch(outgoing, stat):
    group, capacity, width = outgoing.shape
    narrow = lax.axis_size("tp")
    dma = pltpu.SemaphoreType.DMA
    return pl.pallas_call(
        functools.partial(dispatch_kernel, group, narrow, width),
        out_shape=(
            jax.ShapeDtypeStruct((group, capacity, narrow * width), outgoing.dtype),
            jax.ShapeDtypeStruct((narrow,) + stat.shape, stat.dtype),
        ),
        in_specs=[pl.BlockSpec(memory_space=VMEM)] * 2,
        out_specs=[pl.BlockSpec(memory_space=VMEM)] * 2,
        scratch_shapes=[dma((group,))] * 8 + [dma((3,))] * 2 + [dma((2,))],
        compiler_params=pltpu.CompilerParams(collective_id=0, has_side_effects=True),
    )(outgoing, stat)


def return_kernel(group, narrow, width, part_ref, home_ref, pair_buf, far_out, far_in, done, *sems):
    n_s, n_r, f_s, f_r, a_s, a_r, l_s = sems
    me, t, near, far, cross = places(group, narrow)
    sp_peers = [lax.rem(me + o, group) for o in range(1, group)]
    meet([(p, t) for p in sp_peers] + [(me, near), (me, far)])
    order = sp_peers + [me]

    def part(s, column):
        return part_ref.at[s, :, lanes(column, width)]

    def to_near(s, k):
        return remote(
            part(s, near if k == 0 else cross), pair_buf.at[s, k], n_s.at[s, k], n_r.at[s, k], me, near
        )

    def to_far(s):
        return remote(far_out.at[s], far_in.at[s], f_s.at[s], f_r.at[s], me, far)

    def to_home(s):
        return remote(done.at[s], home_ref.at[me], a_s.at[s], a_r.at[me], s, t)

    for s in order:
        to_near(s, 1).start()
        to_near(s, 0).start()
    own = pltpu.make_async_copy(done.at[me], home_ref.at[me], l_s.at[0])

    def finish(s, i):
        to_near(s, 0).wait_recv()
        to_far(s).wait_recv()
        total = part_ref[s, :, lanes(t, width)].astype(jnp.float32)
        total = total + pair_buf[s, 0].astype(jnp.float32) + far_in[s].astype(jnp.float32)
        done[s] = total.astype(done.dtype)
        if i < group - 1:
            to_home(s).start()
        else:
            own.start()

    lag = min(2, group - 1)
    for i, s in enumerate(order):
        to_near(s, 1).wait_recv()
        pair = part_ref[s, :, lanes(far, width)].astype(jnp.float32) + pair_buf[s, 1].astype(jnp.float32)
        far_out[s] = pair.astype(far_out.dtype)
        to_far(s).start()
        if i >= lag:
            finish(order[i - lag], i - lag)
    for i in range(group - lag, group):
        finish(order[i], i)
    own.wait()
    for s in order:
        to_near(s, 0).wait_send()
        to_near(s, 1).wait_send()
        to_far(s).wait_send()
    for s in sp_peers:
        to_home(s).wait_send()
        remote(done.at[s], home_ref.at[s], a_s.at[s], a_r.at[s], s, t).wait_recv()


def return_home(partial):
    group, capacity, whole = partial.shape
    narrow = lax.axis_size("tp")
    width = whole // narrow
    dma = pltpu.SemaphoreType.DMA
    block = (group, capacity, width)
    return pl.pallas_call(
        functools.partial(return_kernel, group, narrow, width),
        out_shape=jax.ShapeDtypeStruct(block, partial.dtype),
        in_specs=[pl.BlockSpec(memory_space=VMEM)],
        out_specs=pl.BlockSpec(memory_space=VMEM),
        scratch_shapes=[
            VMEM((group, 2, capacity, width), partial.dtype),
            VMEM(block, partial.dtype),
            VMEM(block, partial.dtype),
            VMEM(block, partial.dtype),
        ]
        + [dma((group, 2))] * 2
        + [dma((group,))] * 4
        + [dma((1,))],
        compiler_params=pltpu.CompilerParams(collective_id=1, has_side_effects=True),
    )(partial)


def widen_kernel(narrow, width, pieces, mix_ref, full_ref, *sems):
    n_s, n_r, f_s, f_r, m_s, m_r, l_s = sems
    me, t, near, far, cross = places(1, narrow)
    meet([(me, near), (me, far)])
    rows = mix_ref.shape[0] // pieces

    def src(k):
        return mix_ref.at[pl.ds(k * rows, rows)]

    def spot(k, column):
        return full_ref.at[pl.ds(k * rows, rows), lanes(column, width)]

    def to_far(k):
        return remote(src(k), spot(k, t), f_s.at[k], f_r.at[k], me, far)

    def to_near(k):
        return remote(src(k), spot(k, t), n_s.at[k], n_r.at[k], me, near)

    def onward(k):
        return remote(spot(k, far), spot(k, far), m_s.at[k], m_r.at[k], me, near)

    own = pltpu.make_async_copy(mix_ref, full_ref.at[:, lanes(t, width)], l_s.at[0])
    for k in range(pieces):
        to_far(k).start()
    for k in range(pieces):
        to_near(k).start()
    own.start()
    for k in range(pieces):
        to_far(k).wait_recv()
        onward(k).start()
    own.wait()
    for k in range(pieces):
        to_far(k).wait_send()
        to_near(k).wait()
        onward(k).wait()


def widen(mix):
    rows, width = mix.shape
    narrow = lax.axis_size("tp")
    pieces = 4
    dma = pltpu.SemaphoreType.DMA
    return pl.pallas_call(
        functools.partial(widen_kernel, narrow, width, pieces),
        out_shape=jax.ShapeDtypeStruct((rows, narrow * width), mix.dtype),
        in_specs=[pl.BlockSpec(memory_space=VMEM)],
        out_specs=pl.BlockSpec(memory_space=VMEM),
        scratch_shapes=[dma((pieces,))] * 6 + [dma((1,))],
        compiler_params=pltpu.CompilerParams(collective_id=2, has_side_effects=True),
    )(mix)


def tail_kernel(
    group,
    narrow,
    reach,
    parts_ref,
    grad_ref,
    hat_ref,
    stat_ref,
    taps_ref,
    value_ref,
    gate_ref,
    proj_ref,
    dvalue_ref,
    dgate_ref,
    stats,
    next_stats,
    next_grad,
    next_hat,
    extended,
    pair_in,
    pair_sum,
    others,
    *sems,
):
    t_s, t_r, v_s, v_r, h_s, h_r, x_s, x_r, z_s, z_r = sems
    f32 = jnp.float32
    me, t, near, far, cross = places(group, narrow)
    rows, cols = grad_ref.shape
    halo = next_grad.shape[0]
    pairs = group // 2
    parity = lax.rem(me, 2)
    half = me // 2
    partner = me + 1 - 2 * parity
    ahead, behind = lax.rem(me + 1, group), lax.rem(me + group - 1, group)
    siblings = [lax.rem(t + o, narrow) for o in range(1, narrow)]
    alike = [lax.rem(half + o, pairs) for o in range(1, pairs)]
    everyone = [t] + siblings
    meet(
        [(me, p) for p in siblings]
        + [(ahead, p) for p in everyone]
        + [(behind, p) for p in everyone]
        + [(partner, t)]
        + [(2 * q + parity, t) for q in alike]
    )
    sends = []
    for k, p in enumerate(siblings):
        sends.append(remote(stat_ref, stats.at[k], t_s.at[k], t_r.at[k], me, p))
    for k, p in enumerate(everyone):
        sends.append(remote(stat_ref, next_stats.at[k], v_s.at[k], v_r.at[k], behind, p))
    sends.append(remote(grad_ref.at[pl.ds(0, halo)], next_grad, h_s.at[0], h_r.at[0], behind, t))
    sends.append(remote(hat_ref.at[pl.ds(0, halo)], next_hat, h_s.at[1], h_r.at[1], behind, t))
    for c in sends:
        c.start()

    def swap(q):
        return remote(parts_ref.at[2 * q + 1 - parity], pair_in.at[q], x_s.at[q], x_r.at[q], partner, t)

    def scatter(q):
        return remote(pair_sum.at[q], others.at[half], z_s.at[q], z_r.at[half], 2 * q + parity, t)

    order = alike + [half]
    for q in order:
        swap(q).start()
    for c in sends:
        c.wait_recv()

    channels = cols * narrow

    def finished(grad, hat, total, own):
        total = jnp.transpose(total)
        deviation = jnp.transpose(own)[:, 2:3]
        count = grad.shape[0]
        first, second = total[:count, 0:1] / channels, total[:count, 1:2] / channels
        return deviation[:count] * (grad - first - hat * second)

    total = stat_ref[...]
    following = next_stats[0]
    for k in range(narrow - 1):
        total = total + stats[k]
        following = following + next_stats[k + 1]
    extended[pl.ds(0, rows), :] = finished(grad_ref[...], hat_ref[...], total, stat_ref[...])
    beyond = finished(next_grad[...], next_hat[...], following, next_stats[0])
    extended[pl.ds(rows, halo), :] = jnp.where(me == group - 1, jnp.zeros_like(beyond), beyond)

    step = 32
    strips = cols // 128

    def convolve(index, carry):
        start = pl.multiple_of((index // strips) * step, step)
        column = lanes(lax.rem(index, strips), 128)
        total = jnp.zeros((step, 128), f32)
        window = extended[pl.ds(start, step + halo), column]
        for turn in range(8):
            shifted = window if turn == 0 else pltpu.roll(window, step + halo - turn, 0)
            for j in range(turn, reach, 8):
                total = total + taps_ref[reach - 1 - j : reach - j, column] * shifted[j - turn : j - turn + step]
        place = (pl.ds(start, step), column)
        sig = jax.nn.sigmoid(gate_ref[place].astype(f32))
        dvalue_ref[place] = (total * sig).astype(dvalue_ref.dtype)
        dgate_ref[place] = (total * value_ref[place].astype(f32) * sig * (1.0 - sig)).astype(dgate_ref.dtype)
        return carry

    turns = rows // step * strips
    marks = [turns * i // pairs for i in range(pairs + 1)]
    for i, q in enumerate(order):
        lax.fori_loop(marks[i], marks[i + 1], convolve, 0)
        swap(q).wait_recv()
        both = parts_ref[2 * q + parity].astype(f32) + pair_in[q].astype(f32)
        if i < pairs - 1:
            pair_sum[q] = both.astype(pair_sum.dtype)
            scatter(q).start()
        else:
            proj_ref[...] = both
    for q in alike:
        remote(pair_sum.at[q], others.at[q], z_s.at[q], z_r.at[q], 2 * q + parity, t).wait_recv()
    proj = proj_ref[...]
    for q in alike:
        proj = proj + others[q].astype(f32)
    proj_ref[...] = proj
    for c in sends:
        c.wait_send()
    for q in order:
        swap(q).wait_send()
    for q in alike:
        scatter(q).wait_send()


def tail(parts, grad, hat, stat, taps, value_pre, gate_pre):
    group, block, model = parts.shape
    rows, cols = grad.shape
    narrow = lax.axis_size("tp")
    reach = taps.shape[0]
    halo = -(-(reach - 1) // 8) * 8
    pairs = group // 2
    f32 = jnp.float32
    dma = pltpu.SemaphoreType.DMA
    return pl.pallas_call(
        functools.partial(tail_kernel, group, narrow, reach),
        out_shape=(
            jax.ShapeDtypeStruct((block, model), f32),
            jax.ShapeDtypeStruct((rows, cols), value_pre.dtype),
            jax.ShapeDtypeStruct((rows, cols), gate_pre.dtype),
        ),
        in_specs=[pl.BlockSpec(memory_space=VMEM)] * 7,
        out_specs=[pl.BlockSpec(memory_space=VMEM)] * 3,
        scratch_shapes=[
            VMEM((narrow - 1,) + stat.shape, f32),
            VMEM((narrow,) + stat.shape, f32),
            VMEM((halo, cols), f32),
            VMEM((halo, cols), f32),
            VMEM((rows + halo, cols), f32),
            VMEM((pairs, block, model), parts.dtype),
            VMEM((pairs, block, model), parts.dtype),
            VMEM((pairs, block, model), parts.dtype),
            dma((narrow - 1,)),
            dma((narrow - 1,)),
            dma((narrow,)),
            dma((narrow,)),
            dma((2,)),
            dma((2,)),
        ]
        + [dma((pairs,))] * 4,
        compiler_params=pltpu.CompilerParams(collective_id=3, has_side_effects=True),
    )(parts, grad, hat, stat, taps, value_pre, gate_pre)


def per_device(
    cot_out,
    route_ids,
    route_weight,
    expert_inputs,
    w_gate,
    w_up,
    w_down,
    w_proj,
    conv_out,
    channel_norm_gain,
    taps,
    value_pre,
    gate_pre,
):
    group_size = lax.axis_size("sp")
    narrow_size = lax.axis_size("tp")
    tok_rows, local_cols = cot_out.shape
    chosen = route_ids.shape[1]
    slot_rows = expert_inputs.shape[1]
    capacity = slot_rows // group_size
    model_width = expert_inputs.shape[2]
    f32, bf16 = jnp.float32, jnp.bfloat16
    experts = jnp.arange(group_size, dtype=jnp.int32)[None, :]
    hots = [(route_ids[:, k : k + 1] == experts) for k in range(chosen)]
    hot = functools.reduce(jnp.logical_or, hots)
    token = jnp.arange(tok_rows, dtype=jnp.int32)
    before = (token[:, None] > token[None, :]).astype(bf16)
    earlier = jnp.dot(before, hot.astype(bf16), preferred_element_type=f32)
    slots = jnp.arange(slot_rows, dtype=jnp.int32)[None, :]
    picks, scaled = [], []
    for k in range(chosen):
        slot = jnp.sum(jnp.where(hots[k], earlier, 0.0), axis=1).astype(jnp.int32)
        dest = route_ids[:, k] * capacity + slot
        picks.append((dest[:, None] == slots).astype(bf16))
        scaled.append((route_weight[:, k : k + 1] * cot_out.astype(f32)).astype(bf16))
    outgoing = lax.dot_general(
        jnp.concatenate(picks, axis=0),
        jnp.concatenate(scaled, axis=0),
        (((0,), (0,)), ((), ())),
        preferred_element_type=f32,
    ).astype(bf16)
    convolution_filter = conv_out.astype(f32)
    stat = jnp.stack(
        [jnp.sum(convolution_filter, axis=1), jnp.sum(convolution_filter * convolution_filter, axis=1)]
    )
    arrived, stats = dispatch(outgoing.reshape(group_size, capacity, local_cols), stat)
    rows_cot = arrived.reshape(slot_rows, model_width)
    rows_in = expert_inputs[0]
    gate_weight = w_gate[0]
    up_weight = w_up[0]
    down_weight = w_down[0]
    gate_lin = jnp.dot(rows_in, gate_weight, preferred_element_type=f32)
    up_lin = jnp.dot(rows_in, up_weight, preferred_element_type=f32)
    gate_c = jnp.minimum(gate_lin, clamp_limit)
    up_c = jnp.clip(up_lin, -clamp_limit, clamp_limit)
    sigma = jax.nn.sigmoid(swish_alpha * gate_c)
    act = ((up_c + 1.0) * gate_c * sigma).astype(bf16)
    grad_down = jnp.dot(act.T, rows_cot, preferred_element_type=f32).astype(bf16)
    d_act = jnp.dot(rows_cot, down_weight.T, preferred_element_type=f32)
    up_open = ((up_lin > -clamp_limit) & (up_lin < clamp_limit)).astype(f32)
    gate_open = (gate_lin < clamp_limit).astype(f32)
    d_up = (d_act * gate_c * sigma * up_open).astype(bf16)
    d_gate = (
        d_act * (up_c + 1.0) * (sigma + swish_alpha * gate_c * sigma * (1.0 - sigma)) * gate_open
    ).astype(bf16)
    grad_gate_part = jnp.dot(rows_in.T, d_gate, preferred_element_type=f32).astype(bf16)
    grad_up_part = jnp.dot(rows_in.T, d_up, preferred_element_type=f32).astype(bf16)
    partial_value = jnp.dot(d_gate, gate_weight.T, preferred_element_type=f32)
    partial_value = partial_value + jnp.dot(d_up, up_weight.T, preferred_element_type=f32)
    coming = return_home(partial_value.astype(bf16).reshape(group_size, capacity, model_width))
    pick_any = functools.reduce(jnp.add, picks)
    summed = jnp.dot(pick_any, coming.reshape(slot_rows, local_cols), preferred_element_type=f32)
    mix_grad = (cot_out.astype(f32) + summed).astype(bf16)
    mix_full = widen(mix_grad)
    channel_total = local_cols * narrow_size
    first_sum, square_sum = jnp.sum(stats, axis=0)
    channel_mean = (first_sum / channel_total)[:, None]
    var = (square_sum / channel_total)[:, None] - channel_mean * channel_mean
    inverse_deviation = lax.rsqrt(var + norm_epsilon)
    normalized_input = (convolution_filter - channel_mean) * inverse_deviation
    normalized_output = normalized_input * channel_norm_gain[None, :]
    sigma_conv = jax.nn.sigmoid(normalized_output)
    act_conv = (normalized_output * sigma_conv).astype(bf16)
    partial_proj = lax.dot_general(
        act_conv, mix_full, (((0,), (0,)), ((), ())), preferred_element_type=f32
    ).astype(bf16)
    d_act_conv = jnp.dot(mix_full, w_proj.T, preferred_element_type=f32)
    normalized_gradient = (
        d_act_conv
        * sigma_conv
        * (1.0 + normalized_output * (1.0 - sigma_conv))
        * channel_norm_gain[None, :]
    )
    terms = jnp.stack(
        [
            jnp.sum(normalized_gradient, axis=1),
            jnp.sum(normalized_gradient * normalized_input, axis=1),
            inverse_deviation[:, 0],
        ]
    )
    terms = jnp.pad(terms, ((0, 8 - terms.shape[0]), (0, 0)))
    grad_proj, grad_value, grad_gate = tail(
        partial_proj.reshape(group_size, local_cols // group_size, model_width),
        normalized_gradient,
        normalized_input,
        terms,
        taps,
        value_pre,
        gate_pre,
    )
    return (
        grad_gate_part[None],
        grad_up_part[None],
        grad_down[None],
        grad_proj,
        grad_value,
        grad_gate,
    )


def solution(mesh):
    return jax.shard_map(
        per_device,
        mesh=mesh,
        in_specs=(
            P("sp", "tp"),
            P("sp", None),
            P("sp", None),
            P("sp", None, None),
            P("sp", None, "tp"),
            P("sp", None, "tp"),
            P("sp", "tp", None),
            P("tp", None),
            P("sp", "tp"),
            P("tp"),
            P(None, "tp"),
            P("sp", "tp"),
            P("sp", "tp"),
        ),
        out_specs=(
            P("sp", None, "tp"),
            P("sp", None, "tp"),
            P("sp", "tp", None),
            P(("tp", "sp"), None),
            P("sp", "tp"),
            P("sp", "tp"),
        ),
        check_vma=False,
    )
```

```python
import functools

import jax
import jax.numpy as jnp
from jax import lax
from jax.experimental import pallas as pl
from jax.experimental.pallas import tpu as pltpu
from jax.sharding import PartitionSpec as P

clamp_limit = 7.0
swish_alpha = 1.702
norm_epsilon = 1e-05
MESH = pl.DeviceIdType.MESH
VMEM = pltpu.VMEM


def lanes(index, width):
    return pl.ds(pl.multiple_of(index * width, width), width)


def places(group, narrow):
    me, t = lax.axis_index("sp"), lax.axis_index("tp")
    near = t + 1 - 2 * lax.rem(t, 2)
    far = lax.rem(t + narrow // 2, narrow)
    return me, t, near, far, lax.rem(near + narrow // 2, narrow)


def spread(group):
    return sorted(range(1, group), key=lambda o: abs(2 * o - group))


def remote(src, dst, send, recv, sp, tp):
    return pltpu.make_async_remote_copy(
        src_ref=src, dst_ref=dst, send_sem=send, recv_sem=recv, device_id=(sp, tp), device_id_type=MESH
    )


def meet(peers):
    barrier = pltpu.get_barrier_semaphore()
    for sp, tp in peers:
        pl.semaphore_signal(barrier, inc=1, device_id=(sp, tp), device_id_type=MESH)
    pl.semaphore_wait(barrier, len(peers))


def dispatch_kernel(
    group,
    narrow,
    width,
    out_ref,
    stat_ref,
    in_ref,
    gate_ref,
    up_ref,
    rows_ref,
    stats_ref,
    gate_lin_ref,
    up_lin_ref,
    *sems,
):
    a_s, a_r, n_s, n_r, f_s, f_r, m_s, m_r, t_s, t_r, l_s = sems
    me, t, near, far, cross = places(group, narrow)
    sp_peers = [lax.rem(me + o, group) for o in spread(group)]
    meet([(p, t) for p in sp_peers] + [(me, near), (me, far), (me, cross)])

    def spot(s, column):
        return rows_ref.at[s, :, lanes(column, width)]

    def swap(s):
        return remote(out_ref.at[s], spot(me, t), a_s.at[s], a_r.at[me], s, t)

    for p in sp_peers:
        swap(p).start()
    stat_own = pltpu.make_async_copy(stat_ref, stats_ref.at[t], l_s.at[0])
    stat_own.start()
    small = []
    for k, p in enumerate((near, far, cross)):
        c = remote(stat_ref, stats_ref.at[t], t_s.at[k], t_r.at[k], me, p)
        c.start()
        small.append(c)
    own = pltpu.make_async_copy(out_ref.at[me], spot(me, t), l_s.at[1])
    own.start()
    own.wait()
    order = [me] + [lax.rem(me + group - o, group) for o in spread(group)]

    def to_far(s):
        return remote(spot(s, t), spot(s, t), f_s.at[s], f_r.at[s], me, far)

    def to_near(s):
        return remote(spot(s, t), spot(s, t), n_s.at[s], n_r.at[s], me, near)

    def onward(s):
        return remote(spot(s, far), spot(s, far), m_s.at[s], m_r.at[s], me, near)

    def relay(s):
        to_far(s).wait_recv()
        onward(s).start()

    turns = 8
    count = in_ref.shape[0] // turns

    def multiply(piece):
        span = pl.ds(piece * count, count)
        rows = in_ref[span, :]
        gate_lin_ref[span, :] = jnp.dot(rows, gate_ref[...], preferred_element_type=jnp.float32)
        up_lin_ref[span, :] = jnp.dot(rows, up_ref[...], preferred_element_type=jnp.float32)

    lag = min(2, group)
    for i, s in enumerate(order):
        if i > 0:
            remote(out_ref.at[s], spot(s, t), a_s.at[s], a_r.at[s], s, t).wait_recv()
        to_far(s).start()
        to_near(s).start()
        if i >= lag:
            relay(order[i - lag])
        for piece in range(turns * i // group, turns * (i + 1) // group):
            multiply(piece)
    for s in order[group - lag :]:
        relay(s)
    for s in order:
        to_far(s).wait_send()
        to_near(s).wait_send()
        onward(s).wait_send()
        remote(spot(s, near), spot(s, near), n_s.at[s], n_r.at[s], me, near).wait_recv()
        remote(spot(s, cross), spot(s, cross), m_s.at[s], m_r.at[s], me, near).wait_recv()
    for p in sp_peers:
        swap(p).wait_send()
    stat_own.wait()
    for c in small:
        c.wait_send()
        c.wait_recv()


def dispatch(outgoing, stat, rows_in, gate_weight, up_weight):
    group, capacity, width = outgoing.shape
    narrow = lax.axis_size("tp")
    dma = pltpu.SemaphoreType.DMA
    return pl.pallas_call(
        functools.partial(dispatch_kernel, group, narrow, width),
        out_shape=(
            jax.ShapeDtypeStruct((group, capacity, narrow * width), outgoing.dtype),
            jax.ShapeDtypeStruct((narrow,) + stat.shape, stat.dtype),
            jax.ShapeDtypeStruct((rows_in.shape[0], gate_weight.shape[1]), jnp.float32),
            jax.ShapeDtypeStruct((rows_in.shape[0], up_weight.shape[1]), jnp.float32),
        ),
        in_specs=[pl.BlockSpec(memory_space=VMEM)] * 5,
        out_specs=[pl.BlockSpec(memory_space=VMEM)] * 4,
        scratch_shapes=[dma((group,))] * 8 + [dma((3,))] * 2 + [dma((2,))],
        compiler_params=pltpu.CompilerParams(collective_id=0, has_side_effects=True),
    )(outgoing, stat, rows_in, gate_weight, up_weight)


def return_kernel(group, narrow, width, part_ref, home_ref, pair_buf, far_out, far_in, done, *sems):
    n_s, n_r, f_s, f_r, a_s, a_r, l_s = sems
    me, t, near, far, cross = places(group, narrow)
    sp_peers = [lax.rem(me + o, group) for o in spread(group)]
    meet([(p, t) for p in sp_peers] + [(me, near), (me, far)])
    order = sp_peers + [me]

    def part(s, column):
        return part_ref.at[s, :, lanes(column, width)]

    def to_near(s, k):
        return remote(
            part(s, near if k == 0 else cross), pair_buf.at[s, k], n_s.at[s, k], n_r.at[s, k], me, near
        )

    def to_far(s):
        return remote(far_out.at[s], far_in.at[s], f_s.at[s], f_r.at[s], me, far)

    def to_home(s):
        return remote(done.at[s], home_ref.at[me], a_s.at[s], a_r.at[me], s, t)

    for s in order:
        to_near(s, 1).start()
    for s in order:
        to_near(s, 0).start()
    own = pltpu.make_async_copy(done.at[me], home_ref.at[me], l_s.at[0])

    def finish(s, i):
        to_near(s, 0).wait_recv()
        to_far(s).wait_recv()
        total = part_ref[s, :, lanes(t, width)].astype(jnp.float32)
        total = total + pair_buf[s, 0].astype(jnp.float32) + far_in[s].astype(jnp.float32)
        done[s] = total.astype(done.dtype)
        if i < group - 1:
            to_home(s).start()
        else:
            own.start()

    for s in order:
        to_near(s, 1).wait_recv()
        pair = part_ref[s, :, lanes(far, width)].astype(jnp.float32) + pair_buf[s, 1].astype(jnp.float32)
        far_out[s] = pair.astype(far_out.dtype)
        to_far(s).start()
    for i, s in enumerate(order):
        finish(s, i)
    own.wait()
    for s in order:
        to_near(s, 0).wait_send()
        to_near(s, 1).wait_send()
        to_far(s).wait_send()
    for s in sp_peers:
        to_home(s).wait_send()
        remote(done.at[s], home_ref.at[s], a_s.at[s], a_r.at[s], s, t).wait_recv()


def return_home(partial):
    group, capacity, whole = partial.shape
    narrow = lax.axis_size("tp")
    width = whole // narrow
    dma = pltpu.SemaphoreType.DMA
    block = (group, capacity, width)
    return pl.pallas_call(
        functools.partial(return_kernel, group, narrow, width),
        out_shape=jax.ShapeDtypeStruct(block, partial.dtype),
        in_specs=[pl.BlockSpec(memory_space=VMEM)],
        out_specs=pl.BlockSpec(memory_space=VMEM),
        scratch_shapes=[
            VMEM((group, 2, capacity, width), partial.dtype),
            VMEM(block, partial.dtype),
            VMEM(block, partial.dtype),
            VMEM(block, partial.dtype),
        ]
        + [dma((group, 2))] * 2
        + [dma((group,))] * 4
        + [dma((1,))],
        compiler_params=pltpu.CompilerParams(collective_id=1, has_side_effects=True),
    )(partial)


def widen_kernel(narrow, width, pieces, mix_ref, full_ref, *sems):
    n_s, n_r, f_s, f_r, m_s, m_r, l_s = sems
    me, t, near, far, cross = places(1, narrow)
    meet([(me, near), (me, far)])
    rows = mix_ref.shape[0] // pieces

    def src(k):
        return mix_ref.at[pl.ds(k * rows, rows)]

    def spot(k, column):
        return full_ref.at[pl.ds(k * rows, rows), lanes(column, width)]

    def to_far(k):
        return remote(src(k), spot(k, t), f_s.at[k], f_r.at[k], me, far)

    def to_near(k):
        return remote(src(k), spot(k, t), n_s.at[k], n_r.at[k], me, near)

    def onward(k):
        return remote(spot(k, far), spot(k, far), m_s.at[k], m_r.at[k], me, near)

    own = pltpu.make_async_copy(mix_ref, full_ref.at[:, lanes(t, width)], l_s.at[0])
    for k in range(pieces):
        to_far(k).start()
    for k in range(pieces):
        to_near(k).start()
    own.start()
    for k in range(pieces):
        to_far(k).wait_recv()
        onward(k).start()
    own.wait()
    for k in range(pieces):
        to_far(k).wait_send()
        to_near(k).wait()
        onward(k).wait()


def widen(mix):
    rows, width = mix.shape
    narrow = lax.axis_size("tp")
    pieces = 4
    dma = pltpu.SemaphoreType.DMA
    return pl.pallas_call(
        functools.partial(widen_kernel, narrow, width, pieces),
        out_shape=jax.ShapeDtypeStruct((rows, narrow * width), mix.dtype),
        in_specs=[pl.BlockSpec(memory_space=VMEM)],
        out_specs=pl.BlockSpec(memory_space=VMEM),
        scratch_shapes=[dma((pieces,))] * 6 + [dma((1,))],
        compiler_params=pltpu.CompilerParams(collective_id=2, has_side_effects=True),
    )(mix)


def tail_kernel(
    group,
    narrow,
    reach,
    parts_ref,
    grad_ref,
    hat_ref,
    stat_ref,
    taps_ref,
    proj_ref,
    others,
    glu_ref,
    stats,
    next_stats,
    next_grad,
    next_hat,
    extended,
    pair_in,
    pair_sum,
    *sems,
):
    t_s, t_r, v_s, v_r, h_s, h_r, x_s, x_r, z_s, z_r = sems
    f32 = jnp.float32
    me, t, near, far, cross = places(group, narrow)
    rows, cols = grad_ref.shape
    halo = next_grad.shape[0]
    pairs = group // 2
    parity = lax.rem(me, 2)
    half = me // 2
    partner = me + 1 - 2 * parity
    ahead, behind = lax.rem(me + 1, group), lax.rem(me + group - 1, group)
    siblings = [lax.rem(t + o, narrow) for o in range(1, narrow)]
    alike = [lax.rem(half + o, pairs) for o in range(1, pairs)]
    everyone = [t] + siblings
    meet(
        [(me, p) for p in siblings]
        + [(ahead, p) for p in everyone]
        + [(behind, p) for p in everyone]
        + [(partner, t)]
        + [(2 * q + parity, t) for q in alike]
    )
    sends = []
    for k, p in enumerate(siblings):
        sends.append(remote(stat_ref, stats.at[k], t_s.at[k], t_r.at[k], me, p))
    for k, p in enumerate(everyone):
        sends.append(remote(stat_ref, next_stats.at[k], v_s.at[k], v_r.at[k], behind, p))
    sends.append(remote(grad_ref.at[pl.ds(0, halo)], next_grad, h_s.at[0], h_r.at[0], behind, t))
    sends.append(remote(hat_ref.at[pl.ds(0, halo)], next_hat, h_s.at[1], h_r.at[1], behind, t))
    for c in sends:
        c.start()

    def swap(q):
        return remote(parts_ref.at[2 * q + 1 - parity], pair_in.at[q], x_s.at[q], x_r.at[q], partner, t)

    def scatter(q):
        return remote(pair_sum.at[q], others.at[slot_of(half, q)], z_s.at[q], z_r.at[half], 2 * q + parity, t)

    def slot_of(source, target):
        return lax.rem(target - source + pairs, pairs) - 1

    order = alike + [half]
    for q in order:
        swap(q).start()
    for c in sends:
        c.wait_recv()

    channels = cols * narrow

    def finished(grad, hat, total, own):
        total = jnp.transpose(total)
        deviation = jnp.transpose(own)[:, 2:3]
        count = grad.shape[0]
        first, second = total[:count, 0:1] / channels, total[:count, 1:2] / channels
        return deviation[:count] * (grad - first - hat * second)

    total = stat_ref[...]
    following = next_stats[0]
    for k in range(narrow - 1):
        total = total + stats[k]
        following = following + next_stats[k + 1]
    extended[pl.ds(0, rows), :] = finished(grad_ref[...], hat_ref[...], total, stat_ref[...])
    beyond = finished(next_grad[...], next_hat[...], following, next_stats[0])
    extended[pl.ds(rows, halo), :] = jnp.where(me == group - 1, jnp.zeros_like(beyond), beyond)

    step = 32
    strips = cols // 128

    def convolve(index, carry):
        start = pl.multiple_of((index // strips) * step, step)
        column = lanes(lax.rem(index, strips), 128)
        total = jnp.zeros((step, 128), f32)
        window = extended[pl.ds(start, step + halo), column]
        for turn in range(8):
            shifted = window if turn == 0 else pltpu.roll(window, step + halo - turn, 0)
            for j in range(turn, reach, 8):
                total = total + taps_ref[reach - 1 - j : reach - j, column] * shifted[j - turn : j - turn + step]
        glu_ref[pl.ds(start, step), column] = total
        return carry

    turns = rows // step * strips
    marks = [turns * i // pairs for i in range(pairs + 1)]
    for i, q in enumerate(order):
        lax.fori_loop(marks[i], marks[i + 1], convolve, 0)
        swap(q).wait_recv()
        both = parts_ref[2 * q + parity].astype(f32) + pair_in[q].astype(f32)
        if i < pairs - 1:
            pair_sum[q] = both.astype(pair_sum.dtype)
            scatter(q).start()
        else:
            proj_ref[...] = both
    for q in alike:
        remote(pair_sum.at[q], others.at[slot_of(q, half)], z_s.at[q], z_r.at[q], 2 * q + parity, t).wait_recv()
    for c in sends:
        c.wait_send()
    for q in order:
        swap(q).wait_send()
    for q in alike:
        scatter(q).wait_send()


def tail(parts, grad, hat, stat, taps):
    group, block, model = parts.shape
    rows, cols = grad.shape
    narrow = lax.axis_size("tp")
    reach = taps.shape[0]
    halo = -(-(reach - 1) // 8) * 8
    pairs = group // 2
    f32 = jnp.float32
    dma = pltpu.SemaphoreType.DMA
    return pl.pallas_call(
        functools.partial(tail_kernel, group, narrow, reach),
        out_shape=(
            jax.ShapeDtypeStruct((block, model), f32),
            jax.ShapeDtypeStruct((pairs - 1, block, model), parts.dtype),
            jax.ShapeDtypeStruct((rows, cols), f32),
        ),
        in_specs=[pl.BlockSpec(memory_space=VMEM)] * 5,
        out_specs=[pl.BlockSpec(memory_space=VMEM)] * 3,
        scratch_shapes=[
            VMEM((narrow - 1,) + stat.shape, f32),
            VMEM((narrow,) + stat.shape, f32),
            VMEM((halo, cols), f32),
            VMEM((halo, cols), f32),
            VMEM((rows + halo, cols), f32),
            VMEM((pairs, block, model), parts.dtype),
            VMEM((pairs, block, model), parts.dtype),
            dma((narrow - 1,)),
            dma((narrow - 1,)),
            dma((narrow,)),
            dma((narrow,)),
            dma((2,)),
            dma((2,)),
        ]
        + [dma((pairs,))] * 4,
        compiler_params=pltpu.CompilerParams(collective_id=3, has_side_effects=True),
    )(parts, grad, hat, stat, taps)


def per_device(
    cot_out,
    route_ids,
    route_weight,
    expert_inputs,
    w_gate,
    w_up,
    w_down,
    w_proj,
    conv_out,
    channel_norm_gain,
    taps,
    value_pre,
    gate_pre,
):
    group_size = lax.axis_size("sp")
    narrow_size = lax.axis_size("tp")
    tok_rows, local_cols = cot_out.shape
    chosen = route_ids.shape[1]
    slot_rows = expert_inputs.shape[1]
    capacity = slot_rows // group_size
    model_width = expert_inputs.shape[2]
    f32, bf16 = jnp.float32, jnp.bfloat16
    experts = jnp.arange(group_size, dtype=jnp.int32)[None, :]
    hots = [(route_ids[:, k : k + 1] == experts) for k in range(chosen)]
    hot = functools.reduce(jnp.logical_or, hots)
    token = jnp.arange(tok_rows, dtype=jnp.int32)
    before = (token[:, None] > token[None, :]).astype(bf16)
    earlier = jnp.dot(before, hot.astype(bf16), preferred_element_type=f32)
    slots = jnp.arange(slot_rows, dtype=jnp.int32)[None, :]
    picks, scaled = [], []
    for k in range(chosen):
        slot = jnp.sum(jnp.where(hots[k], earlier, 0.0), axis=1).astype(jnp.int32)
        dest = route_ids[:, k] * capacity + slot
        picks.append((dest[:, None] == slots).astype(bf16))
        scaled.append((route_weight[:, k : k + 1] * cot_out.astype(f32)).astype(bf16))
    outgoing = lax.dot_general(
        jnp.concatenate(picks, axis=0),
        jnp.concatenate(scaled, axis=0),
        (((0,), (0,)), ((), ())),
        preferred_element_type=f32,
    ).astype(bf16)
    convolution_filter = conv_out.astype(f32)
    stat = jnp.stack(
        [jnp.sum(convolution_filter, axis=1), jnp.sum(convolution_filter * convolution_filter, axis=1)]
    )
    rows_in = expert_inputs[0]
    gate_weight = w_gate[0]
    up_weight = w_up[0]
    down_weight = w_down[0]
    arrived, stats, gate_lin, up_lin = dispatch(
        outgoing.reshape(group_size, capacity, local_cols), stat, rows_in, gate_weight, up_weight
    )
    rows_cot = arrived.reshape(slot_rows, model_width)
    gate_c = jnp.minimum(gate_lin, clamp_limit)
    up_c = jnp.clip(up_lin, -clamp_limit, clamp_limit)
    sigma = jax.nn.sigmoid(swish_alpha * gate_c)
    act = ((up_c + 1.0) * gate_c * sigma).astype(bf16)
    grad_down = jnp.dot(act.T, rows_cot, preferred_element_type=f32).astype(bf16)
    d_act = jnp.dot(rows_cot, down_weight.T, preferred_element_type=f32)
    up_open = ((up_lin > -clamp_limit) & (up_lin < clamp_limit)).astype(f32)
    gate_open = (gate_lin < clamp_limit).astype(f32)
    d_up = (d_act * gate_c * sigma * up_open).astype(bf16)
    d_gate = (
        d_act * (up_c + 1.0) * (sigma + swish_alpha * gate_c * sigma * (1.0 - sigma)) * gate_open
    ).astype(bf16)
    grad_gate_part = jnp.dot(rows_in.T, d_gate, preferred_element_type=f32).astype(bf16)
    grad_up_part = jnp.dot(rows_in.T, d_up, preferred_element_type=f32).astype(bf16)
    partial_value = jnp.dot(d_gate, gate_weight.T, preferred_element_type=f32)
    partial_value = partial_value + jnp.dot(d_up, up_weight.T, preferred_element_type=f32)
    coming = return_home(partial_value.astype(bf16).reshape(group_size, capacity, model_width))
    pick_any = functools.reduce(jnp.add, picks)
    summed = jnp.dot(pick_any, coming.reshape(slot_rows, local_cols), preferred_element_type=f32)
    mix_grad = (cot_out.astype(f32) + summed).astype(bf16)
    mix_full = widen(mix_grad)
    channel_total = local_cols * narrow_size
    first_sum, square_sum = jnp.sum(stats, axis=0)
    channel_mean = (first_sum / channel_total)[:, None]
    var = (square_sum / channel_total)[:, None] - channel_mean * channel_mean
    inverse_deviation = lax.rsqrt(var + norm_epsilon)
    normalized_input = (convolution_filter - channel_mean) * inverse_deviation
    normalized_output = normalized_input * channel_norm_gain[None, :]
    sigma_conv = jax.nn.sigmoid(normalized_output)
    act_conv = (normalized_output * sigma_conv).astype(bf16)
    partial_proj = lax.dot_general(
        act_conv, mix_full, (((0,), (0,)), ((), ())), preferred_element_type=f32
    ).astype(bf16)
    d_act_conv = jnp.dot(mix_full, w_proj.T, preferred_element_type=f32)
    normalized_gradient = (
        d_act_conv
        * sigma_conv
        * (1.0 + normalized_output * (1.0 - sigma_conv))
        * channel_norm_gain[None, :]
    )
    terms = jnp.stack(
        [
            jnp.sum(normalized_gradient, axis=1),
            jnp.sum(normalized_gradient * normalized_input, axis=1),
            inverse_deviation[:, 0],
        ]
    )
    terms = jnp.pad(terms, ((0, 8 - terms.shape[0]), (0, 0)))
    own_proj, other_proj, d_glu = tail(
        partial_proj.reshape(group_size, local_cols // group_size, model_width),
        normalized_gradient,
        normalized_input,
        terms,
        taps,
    )
    grad_proj = own_proj + jnp.sum(other_proj.astype(f32), axis=0)
    gate_sig = jax.nn.sigmoid(gate_pre.astype(f32))
    grad_value = (d_glu * gate_sig).astype(bf16)
    grad_gate = (d_glu * value_pre.astype(f32) * gate_sig * (1.0 - gate_sig)).astype(bf16)
    return (
        grad_gate_part[None],
        grad_up_part[None],
        grad_down[None],
        grad_proj,
        grad_value,
        grad_gate,
    )


def solution(mesh):
    return jax.shard_map(
        per_device,
        mesh=mesh,
        in_specs=(
            P("sp", "tp"),
            P("sp", None),
            P("sp", None),
            P("sp", None, None),
            P("sp", None, "tp"),
            P("sp", None, "tp"),
            P("sp", "tp", None),
            P("tp", None),
            P("sp", "tp"),
            P("tp"),
            P(None, "tp"),
            P("sp", "tp"),
            P("sp", "tp"),
        ),
        out_specs=(
            P("sp", None, "tp"),
            P("sp", None, "tp"),
            P("sp", "tp", None),
            P(("tp", "sp"), None),
            P("sp", "tp"),
            P("sp", "tp"),
        ),
        check_vma=False,
    )
```

```python
import functools

import jax
import jax.numpy as jnp
from jax import lax
from jax.experimental import pallas as pl
from jax.experimental.pallas import tpu as pltpu
from jax.sharding import PartitionSpec as P

clamp_limit = 7.0
swish_alpha = 1.702
norm_epsilon = 1e-05
MESH = pl.DeviceIdType.MESH
VMEM = pltpu.VMEM


def lanes(index, width):
    return pl.ds(pl.multiple_of(index * width, width), width)


def places(group, narrow):
    me, t = lax.axis_index("sp"), lax.axis_index("tp")
    near = t + 1 - 2 * lax.rem(t, 2)
    far = lax.rem(t + narrow // 2, narrow)
    return me, t, near, far, lax.rem(near + narrow // 2, narrow)


def spread(pairs):
    return sorted(range(1, pairs), key=lambda o: abs(2 * o - pairs))


def around(me, group, sign):
    pairs = group // 2
    half, parity = me // 2, lax.rem(me, 2)
    across = [
        2 * lax.rem(half + pairs + sign * o, pairs) + (parity if side == 0 else 1 - parity)
        for o in spread(pairs)
        for side in range(2)
    ]
    return 2 * half + 1 - parity, across


def remote(src, dst, send, recv, sp, tp):
    return pltpu.make_async_remote_copy(
        src_ref=src, dst_ref=dst, send_sem=send, recv_sem=recv, device_id=(sp, tp), device_id_type=MESH
    )


def meet(peers):
    barrier = pltpu.get_barrier_semaphore()
    for sp, tp in peers:
        pl.semaphore_signal(barrier, inc=1, device_id=(sp, tp), device_id_type=MESH)
    pl.semaphore_wait(barrier, len(peers))


def dispatch_kernel(
    group,
    narrow,
    width,
    out_ref,
    stat_ref,
    in_ref,
    gate_ref,
    up_ref,
    rows_ref,
    stats_ref,
    gate_lin_ref,
    up_lin_ref,
    *sems,
):
    a_s, a_r, n_s, n_r, f_s, f_r, m_s, m_r, t_s, t_r, l_s = sems
    me, t, near, far, cross = places(group, narrow)
    partner, across = around(me, group, 1)
    sp_peers = [partner] + across
    meet([(p, t) for p in sp_peers] + [(me, near), (me, far), (me, cross)])

    def spot(s, column):
        return rows_ref.at[s, :, lanes(column, width)]

    def swap(s):
        return remote(out_ref.at[s], spot(me, t), a_s.at[s], a_r.at[me], s, t)

    for p in sp_peers:
        swap(p).start()
    stat_own = pltpu.make_async_copy(stat_ref, stats_ref.at[t], l_s.at[0])
    stat_own.start()
    small = []
    for k, p in enumerate((near, far, cross)):
        c = remote(stat_ref, stats_ref.at[t], t_s.at[k], t_r.at[k], me, p)
        c.start()
        small.append(c)
    own = pltpu.make_async_copy(out_ref.at[me], spot(me, t), l_s.at[1])
    own.start()
    own.wait()
    order = [me, partner] + around(me, group, -1)[1]

    def to_far(s):
        return remote(spot(s, t), spot(s, t), f_s.at[s], f_r.at[s], me, far)

    def to_near(s):
        return remote(spot(s, t), spot(s, t), n_s.at[s], n_r.at[s], me, near)

    def onward(s):
        return remote(spot(s, far), spot(s, far), m_s.at[s], m_r.at[s], me, near)

    def relay(s):
        to_far(s).wait_recv()
        onward(s).start()

    turns = 8
    count = in_ref.shape[0] // turns

    def multiply(piece):
        span = pl.ds(piece * count, count)
        rows = in_ref[span, :]
        gate_lin_ref[span, :] = jnp.dot(rows, gate_ref[...], preferred_element_type=jnp.float32)
        up_lin_ref[span, :] = jnp.dot(rows, up_ref[...], preferred_element_type=jnp.float32)

    lag = min(2, group)
    for i, s in enumerate(order):
        if i > 0:
            remote(out_ref.at[s], spot(s, t), a_s.at[s], a_r.at[s], s, t).wait_recv()
        to_far(s).start()
        to_near(s).start()
        if i >= lag:
            relay(order[i - lag])
        for piece in range(turns * i // group, turns * (i + 1) // group):
            multiply(piece)
    for s in order[group - lag :]:
        relay(s)
    for s in order:
        to_far(s).wait_send()
        to_near(s).wait_send()
        onward(s).wait_send()
        remote(spot(s, near), spot(s, near), n_s.at[s], n_r.at[s], me, near).wait_recv()
        remote(spot(s, cross), spot(s, cross), m_s.at[s], m_r.at[s], me, near).wait_recv()
    for p in sp_peers:
        swap(p).wait_send()
    stat_own.wait()
    for c in small:
        c.wait_send()
        c.wait_recv()


def dispatch(outgoing, stat, rows_in, gate_weight, up_weight):
    group, capacity, width = outgoing.shape
    narrow = lax.axis_size("tp")
    dma = pltpu.SemaphoreType.DMA
    return pl.pallas_call(
        functools.partial(dispatch_kernel, group, narrow, width),
        out_shape=(
            jax.ShapeDtypeStruct((group, capacity, narrow * width), outgoing.dtype),
            jax.ShapeDtypeStruct((narrow,) + stat.shape, stat.dtype),
            jax.ShapeDtypeStruct((rows_in.shape[0], gate_weight.shape[1]), jnp.float32),
            jax.ShapeDtypeStruct((rows_in.shape[0], up_weight.shape[1]), jnp.float32),
        ),
        in_specs=[pl.BlockSpec(memory_space=VMEM)] * 5,
        out_specs=[pl.BlockSpec(memory_space=VMEM)] * 4,
        scratch_shapes=[dma((group,))] * 8 + [dma((3,))] * 2 + [dma((2,))],
        compiler_params=pltpu.CompilerParams(collective_id=0, has_side_effects=True),
    )(outgoing, stat, rows_in, gate_weight, up_weight)


def return_kernel(group, narrow, width, part_ref, home_ref, pair_buf, far_out, far_in, done, *sems):
    n_s, n_r, f_s, f_r, a_s, a_r, l_s = sems
    me, t, near, far, cross = places(group, narrow)
    partner, across = around(me, group, 1)
    sp_peers = across + [partner]
    meet([(p, t) for p in sp_peers] + [(me, near), (me, far)])
    order = sp_peers + [me]

    def part(s, column):
        return part_ref.at[s, :, lanes(column, width)]

    def to_near(s, k):
        return remote(
            part(s, near if k == 0 else cross), pair_buf.at[s, k], n_s.at[s, k], n_r.at[s, k], me, near
        )

    def to_far(s):
        return remote(far_out.at[s], far_in.at[s], f_s.at[s], f_r.at[s], me, far)

    def to_home(s):
        return remote(done.at[s], home_ref.at[me], a_s.at[s], a_r.at[me], s, t)

    for s in order:
        to_near(s, 1).start()
    for s in order:
        to_near(s, 0).start()
    own = pltpu.make_async_copy(done.at[me], home_ref.at[me], l_s.at[0])

    def finish(s, i):
        to_near(s, 0).wait_recv()
        to_far(s).wait_recv()
        total = part_ref[s, :, lanes(t, width)].astype(jnp.float32)
        total = total + pair_buf[s, 0].astype(jnp.float32) + far_in[s].astype(jnp.float32)
        done[s] = total.astype(done.dtype)
        if i < group - 1:
            to_home(s).start()
        else:
            own.start()

    for s in order:
        to_near(s, 1).wait_recv()
        pair = part_ref[s, :, lanes(far, width)].astype(jnp.float32) + pair_buf[s, 1].astype(jnp.float32)
        far_out[s] = pair.astype(far_out.dtype)
        to_far(s).start()
    for i, s in enumerate(order):
        finish(s, i)
    own.wait()
    for s in order:
        to_near(s, 0).wait_send()
        to_near(s, 1).wait_send()
        to_far(s).wait_send()
    for s in sp_peers:
        to_home(s).wait_send()
        remote(done.at[s], home_ref.at[s], a_s.at[s], a_r.at[s], s, t).wait_recv()


def return_home(partial):
    group, capacity, whole = partial.shape
    narrow = lax.axis_size("tp")
    width = whole // narrow
    dma = pltpu.SemaphoreType.DMA
    block = (group, capacity, width)
    return pl.pallas_call(
        functools.partial(return_kernel, group, narrow, width),
        out_shape=jax.ShapeDtypeStruct(block, partial.dtype),
        in_specs=[pl.BlockSpec(memory_space=VMEM)],
        out_specs=pl.BlockSpec(memory_space=VMEM),
        scratch_shapes=[
            VMEM((group, 2, capacity, width), partial.dtype),
            VMEM(block, partial.dtype),
            VMEM(block, partial.dtype),
            VMEM(block, partial.dtype),
        ]
        + [dma((group, 2))] * 2
        + [dma((group,))] * 4
        + [dma((1,))],
        compiler_params=pltpu.CompilerParams(collective_id=1, has_side_effects=True),
    )(partial)


def widen_kernel(narrow, width, pieces, mix_ref, full_ref, *sems):
    n_s, n_r, f_s, f_r, m_s, m_r, l_s = sems
    me, t, near, far, cross = places(1, narrow)
    meet([(me, near), (me, far)])
    rows = mix_ref.shape[0] // pieces

    def src(k):
        return mix_ref.at[pl.ds(k * rows, rows)]

    def spot(k, column):
        return full_ref.at[pl.ds(k * rows, rows), lanes(column, width)]

    def to_far(k):
        return remote(src(k), spot(k, t), f_s.at[k], f_r.at[k], me, far)

    def to_near(k):
        return remote(src(k), spot(k, t), n_s.at[k], n_r.at[k], me, near)

    def onward(k):
        return remote(spot(k, far), spot(k, far), m_s.at[k], m_r.at[k], me, near)

    own = pltpu.make_async_copy(mix_ref, full_ref.at[:, lanes(t, width)], l_s.at[0])
    for k in range(pieces):
        to_far(k).start()
    for k in range(pieces):
        to_near(k).start()
    own.start()
    for k in range(pieces):
        to_far(k).wait_recv()
        onward(k).start()
    own.wait()
    for k in range(pieces):
        to_far(k).wait_send()
        to_near(k).wait()
        onward(k).wait()


def widen(mix):
    rows, width = mix.shape
    narrow = lax.axis_size("tp")
    pieces = 4
    dma = pltpu.SemaphoreType.DMA
    return pl.pallas_call(
        functools.partial(widen_kernel, narrow, width, pieces),
        out_shape=jax.ShapeDtypeStruct((rows, narrow * width), mix.dtype),
        in_specs=[pl.BlockSpec(memory_space=VMEM)],
        out_specs=pl.BlockSpec(memory_space=VMEM),
        scratch_shapes=[dma((pieces,))] * 6 + [dma((1,))],
        compiler_params=pltpu.CompilerParams(collective_id=2, has_side_effects=True),
    )(mix)


def tail_kernel(
    group,
    narrow,
    reach,
    parts_ref,
    grad_ref,
    hat_ref,
    stat_ref,
    taps_ref,
    proj_ref,
    others,
    glu_ref,
    stats,
    next_stats,
    next_grad,
    next_hat,
    extended,
    pair_in,
    pair_sum,
    *sems,
):
    t_s, t_r, v_s, v_r, h_s, h_r, x_s, x_r, z_s, z_r = sems
    f32 = jnp.float32
    me, t, near, far, cross = places(group, narrow)
    rows, cols = grad_ref.shape
    halo = next_grad.shape[0]
    pairs = group // 2
    parity = lax.rem(me, 2)
    half = me // 2
    partner = me + 1 - 2 * parity
    ahead, behind = lax.rem(me + 1, group), lax.rem(me + group - 1, group)
    siblings = [lax.rem(t + o, narrow) for o in range(1, narrow)]
    alike = [lax.rem(half + o, pairs) for o in spread(pairs)]
    cut = parts_ref.shape[2] // 2
    sides = [pl.ds(h * cut, cut) for h in range(2)]
    everyone = [t] + siblings
    meet(
        [(me, p) for p in siblings]
        + [(ahead, p) for p in everyone]
        + [(behind, p) for p in everyone]
        + [(partner, t)]
        + [(2 * q + parity, t) for q in alike]
    )
    sends = []
    for k, p in enumerate(siblings):
        sends.append(remote(stat_ref, stats.at[k], t_s.at[k], t_r.at[k], me, p))
    for k, p in enumerate(everyone):
        sends.append(remote(stat_ref, next_stats.at[k], v_s.at[k], v_r.at[k], behind, p))
    sends.append(remote(grad_ref.at[pl.ds(0, halo)], next_grad, h_s.at[0], h_r.at[0], behind, t))
    sends.append(remote(hat_ref.at[pl.ds(0, halo)], next_hat, h_s.at[1], h_r.at[1], behind, t))
    for c in sends:
        c.start()

    def swap(q, h):
        side = sides[h]
        return remote(
            parts_ref.at[2 * q + 1 - parity, :, side],
            pair_in.at[q, :, side],
            x_s.at[q, h],
            x_r.at[q, h],
            partner,
            t,
        )

    def passing(source, target, h):
        slot = others.at[slot_of(source, target), :, sides[h]]
        return slot, z_r.at[source, h]

    def scatter(q, h):
        slot, arrival = passing(half, q, h)
        return remote(pair_sum.at[q, :, sides[h]], slot, z_s.at[q, h], arrival, 2 * q + parity, t)

    def slot_of(source, target):
        return lax.rem(target - source + pairs, pairs) - 1

    order = alike + [half]
    for q in order:
        for h in range(2):
            swap(q, h).start()
    for c in sends:
        c.wait_recv()

    channels = cols * narrow

    def finished(grad, hat, total, own):
        total = jnp.transpose(total)
        deviation = jnp.transpose(own)[:, 2:3]
        count = grad.shape[0]
        first, second = total[:count, 0:1] / channels, total[:count, 1:2] / channels
        return deviation[:count] * (grad - first - hat * second)

    total = stat_ref[...]
    following = next_stats[0]
    for k in range(narrow - 1):
        total = total + stats[k]
        following = following + next_stats[k + 1]
    extended[pl.ds(0, rows), :] = finished(grad_ref[...], hat_ref[...], total, stat_ref[...])
    beyond = finished(next_grad[...], next_hat[...], following, next_stats[0])
    extended[pl.ds(rows, halo), :] = jnp.where(me == group - 1, jnp.zeros_like(beyond), beyond)

    step = 32
    strips = cols // 128

    def convolve(index, carry):
        start = pl.multiple_of((index // strips) * step, step)
        column = lanes(lax.rem(index, strips), 128)
        total = jnp.zeros((step, 128), f32)
        window = extended[pl.ds(start, step + halo), column]
        for turn in range(8):
            shifted = window if turn == 0 else pltpu.roll(window, step + halo - turn, 0)
            for j in range(turn, reach, 8):
                total = total + taps_ref[reach - 1 - j : reach - j, column] * shifted[j - turn : j - turn + step]
        glu_ref[pl.ds(start, step), column] = total
        return carry

    turns = rows // step * strips
    marks = [turns * i // (2 * pairs) for i in range(2 * pairs + 1)]
    for i, q in enumerate(order):
        for h in range(2):
            lax.fori_loop(marks[2 * i + h], marks[2 * i + h + 1], convolve, 0)
            swap(q, h).wait_recv()
            both = parts_ref[2 * q + parity, :, sides[h]].astype(f32) + pair_in[q, :, sides[h]].astype(f32)
            if i < pairs - 1:
                pair_sum[q, :, sides[h]] = both.astype(pair_sum.dtype)
                scatter(q, h).start()
            else:
                proj_ref[:, sides[h]] = both
    for q in alike:
        for h in range(2):
            slot, arrival = passing(q, half, h)
            remote(pair_sum.at[q, :, sides[h]], slot, z_s.at[q, h], arrival, 2 * q + parity, t).wait_recv()
    for c in sends:
        c.wait_send()
    for h in range(2):
        for q in order:
            swap(q, h).wait_send()
        for q in alike:
            scatter(q, h).wait_send()


def tail(parts, grad, hat, stat, taps):
    group, block, model = parts.shape
    rows, cols = grad.shape
    narrow = lax.axis_size("tp")
    reach = taps.shape[0]
    halo = -(-(reach - 1) // 8) * 8
    pairs = group // 2
    f32 = jnp.float32
    dma = pltpu.SemaphoreType.DMA
    return pl.pallas_call(
        functools.partial(tail_kernel, group, narrow, reach),
        out_shape=(
            jax.ShapeDtypeStruct((block, model), f32),
            jax.ShapeDtypeStruct((pairs - 1, block, model), parts.dtype),
            jax.ShapeDtypeStruct((rows, cols), f32),
        ),
        in_specs=[pl.BlockSpec(memory_space=VMEM)] * 5,
        out_specs=[pl.BlockSpec(memory_space=VMEM)] * 3,
        scratch_shapes=[
            VMEM((narrow - 1,) + stat.shape, f32),
            VMEM((narrow,) + stat.shape, f32),
            VMEM((halo, cols), f32),
            VMEM((halo, cols), f32),
            VMEM((rows + halo, cols), f32),
            VMEM((pairs, block, model), parts.dtype),
            VMEM((pairs, block, model), parts.dtype),
            dma((narrow - 1,)),
            dma((narrow - 1,)),
            dma((narrow,)),
            dma((narrow,)),
            dma((2,)),
            dma((2,)),
        ]
        + [dma((pairs, 2))] * 4,
        compiler_params=pltpu.CompilerParams(collective_id=3, has_side_effects=True),
    )(parts, grad, hat, stat, taps)


def per_device(
    cot_out,
    route_ids,
    route_weight,
    expert_inputs,
    w_gate,
    w_up,
    w_down,
    w_proj,
    conv_out,
    channel_norm_gain,
    taps,
    value_pre,
    gate_pre,
):
    group_size = lax.axis_size("sp")
    narrow_size = lax.axis_size("tp")
    tok_rows, local_cols = cot_out.shape
    chosen = route_ids.shape[1]
    slot_rows = expert_inputs.shape[1]
    capacity = slot_rows // group_size
    model_width = expert_inputs.shape[2]
    f32, bf16 = jnp.float32, jnp.bfloat16
    experts = jnp.arange(group_size, dtype=jnp.int32)[None, :]
    hots = [(route_ids[:, k : k + 1] == experts) for k in range(chosen)]
    hot = functools.reduce(jnp.logical_or, hots)
    token = jnp.arange(tok_rows, dtype=jnp.int32)
    before = (token[:, None] > token[None, :]).astype(bf16)
    earlier = jnp.dot(before, hot.astype(bf16), preferred_element_type=f32)
    slots = jnp.arange(slot_rows, dtype=jnp.int32)[None, :]
    picks, scaled = [], []
    for k in range(chosen):
        slot = jnp.sum(jnp.where(hots[k], earlier, 0.0), axis=1).astype(jnp.int32)
        dest = route_ids[:, k] * capacity + slot
        picks.append((dest[:, None] == slots).astype(bf16))
        scaled.append((route_weight[:, k : k + 1] * cot_out.astype(f32)).astype(bf16))
    outgoing = lax.dot_general(
        jnp.concatenate(picks, axis=0),
        jnp.concatenate(scaled, axis=0),
        (((0,), (0,)), ((), ())),
        preferred_element_type=f32,
    ).astype(bf16)
    convolution_filter = conv_out.astype(f32)
    stat = jnp.stack(
        [jnp.sum(convolution_filter, axis=1), jnp.sum(convolution_filter * convolution_filter, axis=1)]
    )
    rows_in = expert_inputs[0]
    gate_weight = w_gate[0]
    up_weight = w_up[0]
    down_weight = w_down[0]
    arrived, stats, gate_lin, up_lin = dispatch(
        outgoing.reshape(group_size, capacity, local_cols), stat, rows_in, gate_weight, up_weight
    )
    rows_cot = arrived.reshape(slot_rows, model_width)
    gate_c = jnp.minimum(gate_lin, clamp_limit)
    up_c = jnp.clip(up_lin, -clamp_limit, clamp_limit)
    sigma = jax.nn.sigmoid(swish_alpha * gate_c)
    act = ((up_c + 1.0) * gate_c * sigma).astype(bf16)
    grad_down = jnp.dot(act.T, rows_cot, preferred_element_type=f32).astype(bf16)
    d_act = jnp.dot(rows_cot, down_weight.T, preferred_element_type=f32)
    up_open = ((up_lin > -clamp_limit) & (up_lin < clamp_limit)).astype(f32)
    gate_open = (gate_lin < clamp_limit).astype(f32)
    d_up = (d_act * gate_c * sigma * up_open).astype(bf16)
    d_gate = (
        d_act * (up_c + 1.0) * (sigma + swish_alpha * gate_c * sigma * (1.0 - sigma)) * gate_open
    ).astype(bf16)
    grad_gate_part = jnp.dot(rows_in.T, d_gate, preferred_element_type=f32).astype(bf16)
    grad_up_part = jnp.dot(rows_in.T, d_up, preferred_element_type=f32).astype(bf16)
    partial_value = jnp.dot(d_gate, gate_weight.T, preferred_element_type=f32)
    partial_value = partial_value + jnp.dot(d_up, up_weight.T, preferred_element_type=f32)
    coming = return_home(partial_value.astype(bf16).reshape(group_size, capacity, model_width))
    pick_any = functools.reduce(jnp.add, picks)
    summed = jnp.dot(pick_any, coming.reshape(slot_rows, local_cols), preferred_element_type=f32)
    mix_grad = (cot_out.astype(f32) + summed).astype(bf16)
    mix_full = widen(mix_grad)
    channel_total = local_cols * narrow_size
    first_sum, square_sum = jnp.sum(stats, axis=0)
    channel_mean = (first_sum / channel_total)[:, None]
    var = (square_sum / channel_total)[:, None] - channel_mean * channel_mean
    inverse_deviation = lax.rsqrt(var + norm_epsilon)
    normalized_input = (convolution_filter - channel_mean) * inverse_deviation
    normalized_output = normalized_input * channel_norm_gain[None, :]
    sigma_conv = jax.nn.sigmoid(normalized_output)
    act_conv = (normalized_output * sigma_conv).astype(bf16)
    partial_proj = lax.dot_general(
        act_conv, mix_full, (((0,), (0,)), ((), ())), preferred_element_type=f32
    ).astype(bf16)
    d_act_conv = jnp.dot(mix_full, w_proj.T, preferred_element_type=f32)
    normalized_gradient = (
        d_act_conv
        * sigma_conv
        * (1.0 + normalized_output * (1.0 - sigma_conv))
        * channel_norm_gain[None, :]
    )
    terms = jnp.stack(
        [
            jnp.sum(normalized_gradient, axis=1),
            jnp.sum(normalized_gradient * normalized_input, axis=1),
            inverse_deviation[:, 0],
        ]
    )
    terms = jnp.pad(terms, ((0, 8 - terms.shape[0]), (0, 0)))
    own_proj, other_proj, d_glu = tail(
        partial_proj.reshape(group_size, local_cols // group_size, model_width),
        normalized_gradient,
        normalized_input,
        terms,
        taps,
    )
    grad_proj = own_proj + jnp.sum(other_proj.astype(f32), axis=0)
    gate_sig = jax.nn.sigmoid(gate_pre.astype(f32))
    grad_value = (d_glu * gate_sig).astype(bf16)
    grad_gate = (d_glu * value_pre.astype(f32) * gate_sig * (1.0 - gate_sig)).astype(bf16)
    return (
        grad_gate_part[None],
        grad_up_part[None],
        grad_down[None],
        grad_proj,
        grad_value,
        grad_gate,
    )


def solution(mesh):
    return jax.shard_map(
        per_device,
        mesh=mesh,
        in_specs=(
            P("sp", "tp"),
            P("sp", None),
            P("sp", None),
            P("sp", None, None),
            P("sp", None, "tp"),
            P("sp", None, "tp"),
            P("sp", "tp", None),
            P("tp", None),
            P("sp", "tp"),
            P("tp"),
            P(None, "tp"),
            P("sp", "tp"),
            P("sp", "tp"),
        ),
        out_specs=(
            P("sp", None, "tp"),
            P("sp", None, "tp"),
            P("sp", "tp", None),
            P(("tp", "sp"), None),
            P("sp", "tp"),
            P("sp", "tp"),
        ),
        check_vma=False,
    )
```
